256 devices in a mesh: ep: 64 (over z, y, core), tp: 4 (over x).
Axes of the slice: x: 4, y: 4, z: 8, core: 2. Of those that a mesh axis runs over, the one named last changes fastest.
Arguments:
- conv_value: bfloat16 [24576, 2048], P('ep', 'tp'), may hold values from -36 to 36
- conv_gate: bfloat16 [24576, 2048], P('ep', 'tp'), may hold values from -8 to 8
- conv_taps: bfloat16 [31, 2048], P(None, 'tp'), may hold values from -1 to 1
- conv_gain: float32 [2048], P('tp'), may hold values from 0.1 to 1.9
- conv_proj: bfloat16 [2048, 2048], P('tp'), may hold values from -0.125 to 0.125
- moe_tokens: bfloat16 [24576, 2048], P('ep'), may hold values from -6 to 6
- moe_gain: float32 [2048], replicated, may hold values from 0.1 to 1.9
- routes: int32 [24576, 2], P('ep'), may hold values from 0 to 63, all different within a row; in each aligned block of 384 rows (0 to 383, 384 to 767, ...) at most 18 rows name the same one
- route_weights: float32 [24576, 2], P('ep'), may hold values from 0.3 to 3
- expert_gate: bfloat16 [64, 2048, 1024], P('ep', None, 'tp'), may hold values from -0.125 to 0.125
- expert_up: bfloat16 [64, 2048, 1024], P('ep', None, 'tp'), may hold values from -0.125 to 0.125
- expert_down: bfloat16 [64, 1024, 2048], P('ep', 'tp'), may hold values from -0.1875 to 0.1875
- shared_gate: bfloat16 [2048, 256], replicated, may hold values from -0.125 to 0.125
- shared_up: bfloat16 [2048, 256], replicated, may hold values from -0.125 to 0.125
- shared_down: bfloat16 [256, 2048], P(None, 'tp'), may hold values from -0.375 to 0.375
Outputs:
- conv_result: bfloat16 [24576, 2048], P('ep', 'tp')
- moe_result: bfloat16 [24576, 2048], P('ep', 'tp')
The draws below stay inside these ranges and needn't reach their ends.
Inputs may be any that keep to these rules, and one draw needn't show every extreme that they name: `routes`: each row names 2 different experts. Among the 384 rows of one index of ep (aligned blocks in order) no expert is named more than 18 times, and in some blocks one expert is named exactly 18 times.
All inputs are finite; a program needn't handle non-finite values.
Results may differ from the reference program's by a relative error of at most 0.01.
Values may be sent and summed in bfloat16 or wider, within the bound.
A program may use at most 64 MiB of HBM per device.

```python
import math
import jax
import jax.numpy as jnp
import numpy as np
from jax import lax

D = 2048
KERNEL = 31
EXPERT_FF = 1024
SHARED_FF = 256
TOPK = 2
TOK_DEV = 384
TOKENS = 24576
EXPERTS = 64
CAPACITY = 18
N_EP = 64
N_TP = 4


def draw_conv_value(key, part):
    first, second = jax.random.split(jax.random.fold_in(key, 11))
    position = jnp.arange(D, dtype=jnp.float32) / (D - 1)
    rough = jnp.exp(jax.random.uniform(second, (D,), jnp.float32, -0.35, 0.35))
    column_scale = jnp.exp(jnp.log(0.5) + position * jnp.log(8.0)) * rough
    values = jnp.clip(jax.random.normal(first, (TOKENS, D), jnp.float32), -6.0, 6.0)
    return (values * column_scale[None, :]).astype(jnp.bfloat16)


def levels(own_key, extent, pieces, low, largest):
    level, own = 1.0, jax.random.fold_in(own_key, 6)
    for dim, blocks in pieces:
        draws = jnp.exp(jax.random.uniform(jax.random.fold_in(own, dim), (blocks,), jnp.float32, low / len(pieces), largest / len(pieces)))
        level = level * jnp.repeat(draws, extent[dim] // blocks).reshape([-1 if axis == dim else 1 for axis in range(len(extent))])
    return level


def shared_out(key, own, number, rows, amount, top, most, lean):
    ranking = jax.random.permutation(key, amount)
    packed, ordinary = portions_of(amount, rows * top, most, lean, True), portions_of(amount, rows * top, most, lean, False)
    places = jnp.arange(amount)

    def named(lengths, turn):
        used = int((lengths > 0).sum())
        fixed = max(1, used // 4)
        shifted = fixed + (places - fixed + turn * (used - fixed)) % max(1, amount - fixed)
        return jnp.zeros((amount,), jnp.int32).at[ranking[jnp.where(places < fixed, places, shifted)]].set(jnp.asarray(lengths, jnp.int32))

    lengths = jnp.where(number % 4 == 0, named(packed, number // 4), named(ordinary, number - number // 4 - 1))
    mixed = jax.random.permutation(jax.random.fold_in(own, 3), amount)
    donor, taker = mixed[0:amount // 2 * 2:2], mixed[1:amount // 2 * 2:2]
    room = jnp.minimum(lengths[donor] - 1, most - lengths[taker]) // 2
    room = jnp.where((donor == ranking[0]) | (taker == ranking[0]) | (lengths[taker] == 0), 0, jnp.maximum(room, 0))
    shifted = jax.random.randint(jax.random.fold_in(own, 4), (amount // 2,), 0, 1 << 20) % (room + 1)
    lengths = lengths.at[donor].add(-shifted).at[taker].add(shifted)
    members = jnp.searchsorted(jnp.cumsum(lengths), jnp.arange(rows * top), side="right").astype(jnp.int32)
    table = members.reshape(top, rows).T
    table = table[jax.random.permutation(jax.random.fold_in(own, 1), rows)]
    turn = jax.random.randint(jax.random.fold_in(own, 2), (rows, 1), 0, top)
    return jnp.take_along_axis(table, (jnp.arange(top)[None, :] + turn) % top, axis=1)


def portions_of(amount, total, reach, skew, full):
    portions = [(1 << 20) // math.isqrt(grade ** skew) + 1 for grade in range(1, amount + 1)]
    largest = reach if full else min(reach, max(-(-total // amount), total * portions[0] // sum(portions)))
    least = 1 if total - largest >= amount - 1 else 0
    given, spare = [largest] + [least] * (amount - 1), total - largest - least * (amount - 1)
    while spare > 0:
        movable = [i for i in range(1, amount) if given[i] < largest] or [i for i in range(1, amount) if given[i] < reach]
        mass, budget = sum([portions[i] for i in movable]), spare
        for i in movable:
            extra = min(reach - given[i], max(1, budget * portions[i] // mass), spare)
            given[i] = given[i] + extra
            spare = spare - extra
    return np.array(given)


def normal_values(stream_key, dims, deviation, limit, shards=(), kind=jnp.bfloat16):
    values = jax.random.normal(stream_key, dims, jnp.float32) * deviation
    if len(shards) > 0:
        values = levels(stream_key, dims, shards, -0.22, 0.18) * values
    return jnp.clip(values, min=-limit, max=limit).astype(kind)


def setup_inputs(seed: int = 0) -> dict:
    streams_of = jax.random.split(jax.random.key(seed), 16)
    conv_value = draw_conv_value(jax.random.fold_in(streams_of[15], 71), 0)
    conv_gate = normal_values(streams_of[1], (TOKENS, D), 1.5, 8.0, ((0, 64), (1, 4)))
    conv_taps = normal_values(streams_of[2], (KERNEL, D), KERNEL ** -0.5, 1.0, ((1, 4),))
    conv_gain = jnp.clip(1.0 + 0.18 * jax.random.normal(streams_of[3], (D,), jnp.float32), 0.1, 1.9)
    conv_proj = normal_values(streams_of[4], (D, D), D ** -0.5, 0.125, ((0, 4),))
    moe_tokens = normal_values(streams_of[5], (TOKENS, D), 1.0, 6.0, ((0, 64),))
    moe_gain = jnp.clip(1.0 + 0.18 * jax.random.normal(streams_of[6], (D,), jnp.float32), 0.1, 1.9)
    routes_keys = jax.random.split(jax.random.fold_in(streams_of[7], 1), TOKENS // TOK_DEV)
    routes_turns = jax.random.permutation(jax.random.fold_in(streams_of[7], 3), TOKENS // TOK_DEV)
    routes = jax.vmap(lambda own, number: shared_out(jax.random.fold_in(streams_of[7], 2), own, number, TOK_DEV, EXPERTS, TOPK, CAPACITY, 1))(routes_keys, routes_turns).reshape((TOKENS, TOPK))
    route_weights = jnp.clip(jnp.exp(math.log(3.0) - 2.3025851 * jax.random.uniform(streams_of[8], (TOKENS, TOPK), jnp.float32) ** levels(streams_of[8], (TOKENS, TOPK), ((0, 64),), -0.2, 0.2)), 0.3, 3.0)
    expert_gate = normal_values(streams_of[9], (EXPERTS, D, EXPERT_FF), D ** -0.5, 0.125, ((0, 64), (2, 4)))
    expert_up = normal_values(streams_of[10], (EXPERTS, D, EXPERT_FF), D ** -0.5, 0.125, ((0, 64), (2, 4)))
    expert_down = normal_values(streams_of[11], (EXPERTS, EXPERT_FF, D), EXPERT_FF ** -0.5, 0.1875, ((0, 64), (1, 4)))
    shared_gate = normal_values(streams_of[12], (D, SHARED_FF), D ** -0.5, 0.125)
    shared_up = normal_values(streams_of[13], (D, SHARED_FF), D ** -0.5, 0.125)
    shared_down = normal_values(streams_of[14], (SHARED_FF, D), SHARED_FF ** -0.5, 0.375, ((1, 4),))
    return {"conv_value": conv_value, "conv_gate": conv_gate, "conv_taps": conv_taps, "conv_gain": conv_gain, "conv_proj": conv_proj, "moe_tokens": moe_tokens, "moe_gain": moe_gain, "routes": routes, "route_weights": route_weights, "expert_gate": expert_gate, "expert_up": expert_up, "expert_down": expert_down, "shared_gate": shared_gate, "shared_up": shared_up, "shared_down": shared_down}


epsilon = 1e-05

def rounded_block(product):
    return lax.optimization_barrier(product.astype(jnp.bfloat16)).astype(jnp.float32)

def reference(conv_value, conv_gate, conv_taps, conv_gain, conv_proj, moe_tokens, moe_gain, routes, route_weights, expert_gate, expert_up, expert_down, shared_gate, shared_up, shared_down):
    gated_rows = (conv_value.astype(jnp.float32) * jax.nn.sigmoid(conv_gate.astype(jnp.float32))).astype(jnp.bfloat16)
    padded = jnp.concatenate([jnp.zeros((KERNEL - 1, D), jnp.bfloat16), gated_rows], axis=0).astype(jnp.float32)
    tap_weights = conv_taps.astype(jnp.float32)
    convolved = jnp.zeros((TOKENS, D), jnp.float32)
    for offset in range(KERNEL):
        convolved = convolved + tap_weights[offset][None, :] * padded[offset:offset + TOKENS]
    average = lax.optimization_barrier(jnp.sum(convolved, axis=1)) / D
    variance = lax.optimization_barrier(jnp.sum(convolved * convolved, axis=1)) / D - average * average
    scaled = (convolved - average[:, None]) * lax.rsqrt(variance + epsilon)[:, None] * conv_gain[None, :]
    activated = jax.nn.silu(scaled).astype(jnp.bfloat16)
    block_width = D // N_TP
    conv_total = jnp.zeros((TOKENS, D), jnp.float32)
    for block in range(N_TP):
        product = jnp.dot(activated[:, block * block_width:(block + 1) * block_width], conv_proj[block * block_width:(block + 1) * block_width], preferred_element_type=jnp.float32)
        conv_total = conv_total + rounded_block(product)
    conv_result = conv_total.astype(jnp.bfloat16)
    tokens = moe_tokens.astype(jnp.float32)
    token_mean = lax.optimization_barrier(jnp.mean(tokens, axis=1, keepdims=True))
    centered = tokens - token_mean
    token_var = lax.optimization_barrier(jnp.mean(centered * centered, axis=1, keepdims=True))
    normalized = (centered * lax.rsqrt(token_var + epsilon) * moe_gain[None, :]).astype(jnp.bfloat16)
    shared_hidden = (jax.nn.silu(jnp.dot(normalized, shared_gate, preferred_element_type=jnp.float32)) * jnp.dot(normalized, shared_up, preferred_element_type=jnp.float32)).astype(jnp.bfloat16)
    shared_part = jnp.dot(shared_hidden, shared_down, preferred_element_type=jnp.float32)
    entries = TOKENS * TOPK
    flat_routes = routes.reshape(-1).astype(jnp.int32)
    flat_index = jnp.arange(entries, dtype=jnp.int32)
    slot_count = N_EP * CAPACITY
    hidden_width = EXPERT_FF // N_TP

    def one_expert(carried, expert):
        chosen = (flat_routes == expert).astype(jnp.int32)
        order = (jnp.cumsum(chosen) - chosen).astype(jnp.int32)
        target = jnp.where(chosen > 0, order, slot_count).astype(jnp.int32)
        source_row = jnp.zeros((slot_count,), jnp.int32).at[target].set(flat_index, mode='drop')
        filled = jnp.zeros((slot_count,), jnp.int32).at[target].set(jnp.ones((entries,), jnp.int32), mode='drop')
        rows_in = normalized[(source_row // TOPK).astype(jnp.int32)]
        hidden = (jax.nn.silu(jnp.dot(rows_in, expert_gate[expert], preferred_element_type=jnp.float32)) * jnp.dot(rows_in, expert_up[expert], preferred_element_type=jnp.float32)).astype(jnp.bfloat16)
        down_rows = expert_down[expert]
        total = jnp.zeros((slot_count, D), jnp.float32)
        for block in range(N_TP):
            product = jnp.dot(hidden[:, block * hidden_width:(block + 1) * hidden_width], down_rows[block * hidden_width:(block + 1) * hidden_width], preferred_element_type=jnp.float32)
            total = total + rounded_block(product)
        write_at = jnp.where(filled > 0, source_row, entries).astype(jnp.int32)
        carried = carried.at[write_at].set(total.astype(jnp.bfloat16), mode='drop')
        return (carried, None)
    expert_rows, _ = lax.scan(one_expert, jnp.zeros((entries, D), jnp.bfloat16), jnp.arange(EXPERTS, dtype=jnp.int32))
    expert_rows = expert_rows.reshape(TOKENS, TOPK, D)
    moe_total = shared_part
    for choice_index in range(TOPK):
        moe_total = moe_total + route_weights[:, choice_index][:, None] * expert_rows[:, choice_index].astype(jnp.float32)
    moe_result = moe_total.astype(jnp.bfloat16)
    return (conv_result, moe_result)
```

```python
import functools

import jax
import jax.numpy as jnp
from jax import lax
from jax.experimental import pallas as pl
from jax.experimental.pallas import tpu as pltpu
from jax.sharding import PartitionSpec as P

MESH = pl.DeviceIdType.MESH
F32 = jnp.float32
BF16 = jnp.bfloat16
epsilon = 1e-05

ORDER = (0, 1, 7, 2, 6, 3, 5, 4)
PLANE = 8
MAIN = 16
REST = 2
ROWS = PLANE * (MAIN + REST)
BODY = PLANE * MAIN
NEAR = 3
BATCHES = ((0, 3), (7, 1), (5, 2), (3, 2))


def silu(v):
    return v / (1.0 + jnp.exp(-v))


def dot(a, b):
    return jnp.dot(a, b, preferred_element_type=F32)


def iota(shape, dim):
    return lax.broadcasted_iota(jnp.int32, shape, dim)


def kernel(
    cv_hbm,
    cg_hbm,
    taps_ref,
    cgain_ref,
    cproj_hbm,
    tok_hbm,
    mgain_ref,
    routes_ref,
    weights_ref,
    eg_hbm,
    eu_hbm,
    ed_hbm,
    sg_hbm,
    su_hbm,
    sd_hbm,
    conv_out,
    moe_out,
    cv,
    cg,
    cproj,
    tok,
    wg,
    wu,
    sg,
    su,
    sd,
    norm,
    send_near,
    send_near_rest,
    send_far,
    send_far_rest,
    xin,
    in_near_rest,
    in_far_rest,
    hid,
    down,
    down_pass,
    back_send,
    back_send_rest,
    back,
    back_rest,
    total,
    padded,
    taps,
    conv,
    ssum,
    ssq,
    tail,
    halo,
    stat_send,
    stat,
    act,
    cfar,
    cright,
    cleft,
    cown,
    half_a,
    half_b,
    from_left,
    from_right,
    load_sem,
    go_send,
    go_recv,
    go_rest_send,
    go_rest_recv,
    back_ssem,
    back_rsem,
    back_rest_ssem,
    back_rest_rsem,
    ag_send,
    ag_recv,
    down_send,
    down_recv,
    halo_send,
    halo_recv,
    stat_ssem,
    stat_rsem,
    rs_send,
    rs_recv,
):
    ep, tp = lax.axis_index("ep"), lax.axis_index("tp")
    n_ep, n_tp = lax.axis_size("ep"), lax.axis_size("tp")
    planes = n_ep // PLANE
    z, mine = ep // PLANE, lax.rem(ep, PLANE)
    right, left, across = (lax.rem(tp + i, n_tp) for i in (1, 3, 2))
    tokens, width = tok.shape
    quarter = width // n_tp
    ff = wg.shape[1]

    def remote(src, dst, ssem, rsem, to_ep, to_tp):
        return pltpu.make_async_remote_copy(
            src_ref=src,
            dst_ref=dst,
            send_sem=ssem,
            recv_sem=rsem,
            device_id=(to_ep, to_tp),
            device_id_type=MESH,
        )

    def arrived(ref, sem):
        remote(ref, ref, sem, sem, ep, right).wait_recv()

    def left_here(ref, sem):
        remote(ref, ref, sem, sem, ep, right).wait_send()

    barrier = pltpu.get_barrier_semaphore()

    @pl.loop(1, n_ep)
    def _(o):
        pl.semaphore_signal(
            barrier, inc=1, device_id=(lax.rem(ep + o, n_ep), tp), device_id_type=MESH
        )

    for peer in (right, left, across):
        pl.semaphore_signal(barrier, inc=1, device_id=(ep, peer), device_id_type=MESH)

    def at_quarter(q):
        return pl.ds(pl.multiple_of(q * quarter, quarter), quarter)

    def at_ff(q):
        return pl.ds(pl.multiple_of(q * ff, ff), ff)

    loads = {}
    for number, (name, src, dst) in enumerate(
        (
            ("tok", tok_hbm, tok),
            ("cv", cv_hbm, cv),
            ("cg", cg_hbm, cg),
            ("sg", sg_hbm, sg),
            ("su", su_hbm, su),
            ("sd", sd_hbm, sd),
            ("cproj", cproj_hbm, cproj),
            ("wg", eg_hbm.at[0], wg),
            ("wu", eu_hbm.at[0], wu),
            ("down", ed_hbm.at[0, :, at_quarter(tp)], down.at[at_ff(tp)]),
        )
    ):
        loads[name] = pltpu.make_async_copy(src, dst, load_sem.at[number])
        loads[name].start()

    loads["cv"].wait()
    loads["cg"].wait()
    blocks = quarter // 128
    extra = halo.shape[0]
    for b in range(blocks):
        lanes = slice(b * 128, (b + 1) * 128)
        gated = (cv[:, lanes].astype(F32) * jax.nn.sigmoid(cg[:, lanes].astype(F32))).astype(BF16)
        padded[b, extra:, :] = gated.astype(F32)
        tail[:, lanes] = gated[tokens - extra :]
        taps[b, 0:31] = taps_ref[:, lanes].astype(F32)

    loads["tok"].wait()
    for r in range(0, tokens, 64):
        rows = tok[r : r + 64, :].astype(F32)
        mean = jnp.sum(rows, axis=1, keepdims=True) * (1.0 / width)
        centered = rows - mean
        var = jnp.sum(centered * centered, axis=1, keepdims=True) * (1.0 / width)
        norm[r : r + 64, :] = (centered * lax.rsqrt(var + epsilon) * mgain_ref[...]).astype(BF16)

    pl.semaphore_wait(barrier, n_ep - 1 + n_tp - 1)

    next_ep = lax.rem(ep + 1, n_ep)
    remote(tail, halo, halo_send, halo_recv, next_ep, tp).start()

    half = ff // 2

    def down_rows(owner, first, count):
        return down.at[pl.ds(pl.multiple_of(owner * ff + first, half), count)]

    ed = ed_hbm.at[0]
    remote(ed.at[:, at_quarter(right)], down_rows(tp, 0, ff), down_send.at[0], down_recv.at[0], ep, right).start()
    remote(ed.at[:, at_quarter(left)], down_rows(tp, 0, ff), down_send.at[1], down_recv.at[1], ep, left).start()
    remote(ed.at[0:half, at_quarter(across)], down_pass.at[0], down_send.at[2], down_recv.at[2], ep, right).start()
    remote(ed.at[half:ff, at_quarter(across)], down_pass.at[1], down_send.at[3], down_recv.at[3], ep, left).start()

    routes = routes_ref[...]
    first, second = routes[0:1, :], routes[1:2, :]
    names = iota((n_ep, tokens), 0)
    is_first = (names == first).astype(F32)
    is_second = (names == second).astype(F32)
    earlier = (iota((tokens, tokens), 0) < iota((tokens, tokens), 1)).astype(F32).astype(BF16)
    before = dot((is_first + is_second).astype(BF16), earlier)

    def slot_of(route, chosen):
        rank = jnp.sum(before * chosen, axis=0, keepdims=True).astype(jnp.int32)
        away = ((route >> 3) - z + planes) & (planes - 1)
        place = route & (PLANE - 1)
        group = jnp.where(away == 0, 0, jnp.where(away <= 4, 2 * away - 1, 2 * (planes - away)))
        inside = jnp.where(rank < MAIN, place * MAIN + rank, BODY + place * REST + rank - MAIN)
        return group * ROWS + inside

    slot_first, slot_second = slot_of(first, is_first), slot_of(second, is_second)

    way = iota((64, 64), 0)
    here = iota((64, 64), 1)
    same = (way >> 3 == (here >> 1 & 7)) & ((way >> 1 & 3) == here >> 4) & ((way & 1) == (here & 1))
    to_way = same.astype(F32).astype(BF16)
    way = iota((64, 64), 1)
    here = iota((64, 64), 0)
    same = (way >> 3 == (here >> 1 & 7)) & ((way >> 1 & 3) == here >> 4) & ((way & 1) == (here & 1))
    to_here = same.astype(F32).astype(BF16)

    def pack_rest(rest):
        n = rest.shape[1] // 512
        stacked = jnp.concatenate(
            [
                jnp.concatenate(
                    [rest[:, q * 512 + g * 128 : q * 512 + (g + 1) * 128] for q in range(n)], axis=1
                )
                for g in range(4)
            ],
            axis=0,
        )
        return dot(to_way, stacked.astype(BF16)).reshape(8, 8, n * 128)

    def unpack_rest(packed):
        n = packed.shape[2] // 128
        stacked = dot(to_here, packed.astype(F32).reshape(64, n * 128).astype(BF16))
        return jnp.concatenate(
            [
                stacked[g * 16 : (g + 1) * 16, q * 128 : (q + 1) * 128]
                for q in range(n)
                for g in range(4)
            ],
            axis=1,
        ).astype(BF16)

    def row_of(group, place, count=MAIN):
        return pl.ds(pl.multiple_of(group * ROWS + place * MAIN, MAIN), count)

    def place_rows(place):
        return pl.ds(pl.multiple_of(place * MAIN, MAIN), MAIN)

    def exchange(group, sign, main, main_at, rest, rest_at, ssem, rsem, rest_ssem, rest_rsem):
        plane = lax.rem(z + sign * ORDER[group] + planes, planes)

        @pl.loop(1 if group == 0 else 0, PLANE)
        def _(o):
            place = lax.rem(mine + o, PLANE)
            to = plane * PLANE + place
            remote(main.at[place_rows(place)], main_at, ssem.at[group], rsem.at[group], to, tp).start()
            remote(rest.at[place], rest_at, rest_ssem.at[group], rest_rsem.at[group], to, tp).start()

    def sent_or_come(group, wait, main, rest, sem, rest_sem):
        count = PLANE - 1 if group == 0 else PLANE
        wait(main.at[0 : count * MAIN], sem.at[group])
        wait(rest.at[0:count], rest_sem.at[group])

    def far_lanes():
        return at_quarter(tp)

    for group in (0, 1, 2, 7, 5, 6, 3, 4):
        row = iota((ROWS, tokens), 0) + group * ROWS
        pick = ((row == slot_first) | (row == slot_second)).astype(F32).astype(BF16)
        if group < NEAR:
            rows = dot(pick, norm[...])
            send_near[group] = rows[0:BODY].astype(BF16)
            send_near_rest[group] = pack_rest(rows[BODY:]).astype(BF16)
            main, rest = send_near.at[group], send_near_rest.at[group]
            main_at, rest_at = xin.at[row_of(group, mine)], in_near_rest.at[group, mine]
        else:
            rows = dot(pick, norm[:, far_lanes()])
            send_far[group - NEAR] = rows[0:BODY].astype(BF16)
            send_far_rest[group - NEAR] = pack_rest(rows[BODY:]).astype(BF16)
            main, rest = send_far.at[group - NEAR], send_far_rest.at[group - NEAR]
            main_at = xin.at[row_of(group, mine), far_lanes()]
            rest_at = in_far_rest.at[group - NEAR, mine]
        exchange(group, 1, main, main_at, rest, rest_at, go_send, go_recv, go_rest_send, go_rest_recv)
        if group == 0:
            xin[row_of(0, mine), :] = send_near[0, place_rows(mine), :]
            in_near_rest[0, mine] = send_near_rest[0, mine]

    arrived(halo, halo_recv)
    for b in range(blocks):
        before_rows = halo[:, b * 128 : (b + 1) * 128].astype(F32)
        padded[b, 0:extra, :] = jnp.where(ep == 0, jnp.zeros_like(before_rows), before_rows)
    ssum[...] = jnp.zeros_like(ssum)
    ssq[...] = jnp.zeros_like(ssq)

    @pl.loop(0, blocks)
    def _(b):
        for r in range(0, tokens, 64):
            acc = jnp.zeros((64, 128), F32)
            for offset in range(31):
                start = r + offset + extra - 30
                acc = acc + taps[b, offset : offset + 1, :] * padded[b, start : start + 64, :]
            conv[b, r : r + 64, :] = acc
            ssum[r : r + 64, :] += acc
            ssq[r : r + 64, :] += acc * acc

    eighth = iota((8, tokens), 0)
    sums = jnp.sum(ssum[...].T, axis=0, keepdims=True)
    squares = jnp.sum(ssq[...].T, axis=0, keepdims=True)
    own_stat = jnp.where(eighth == 0, sums, jnp.where(eighth == 1, squares, 0.0))
    stat_send[...] = own_stat
    stat[tp] = own_stat
    for i, peer in enumerate((right, left, across)):
        remote(stat_send, stat.at[tp], stat_ssem.at[i], stat_rsem.at[i], ep, peer).start()

    loads["sg"].wait()
    loads["su"].wait()
    loads["sd"].wait()
    shared = (silu(dot(norm[...], sg[...])) * dot(norm[...], su[...])).astype(BF16)
    total[...] = dot(shared, sd[...])

    for i, peer in enumerate((left, right, across)):
        arrived(stat.at[peer], stat_rsem.at[i])
    sums = stat[0] + stat[1] + stat[2] + stat[3]
    average = sums[0:1] * (1.0 / width)
    variance = sums[1:2] * (1.0 / width) - average * average
    scale = lax.rsqrt(variance + epsilon)
    tall = iota((128, tokens), 0)
    turned = jnp.where(tall == 0, average, jnp.where(tall == 1, scale, 0.0)).T
    average, scale = turned[:, 0:1], turned[:, 1:2]
    for b in range(blocks):
        lanes = slice(b * 128, (b + 1) * 128)
        act[:, lanes] = silu((conv[b] - average) * scale * cgain_ref[:, lanes]).astype(BF16)

    loads["cproj"].wait()
    upper = tokens // 2
    top, bottom = slice(0, upper), slice(upper, tokens)

    def product(q):
        return dot(act[...], cproj[:, at_quarter(q)])

    cfar[...] = product(across).astype(BF16)
    remote(cfar.at[top], half_a, rs_send.at[0], rs_recv.at[0], ep, right).start()
    remote(cfar.at[bottom], half_b, rs_send.at[1], rs_recv.at[1], ep, left).start()
    cright[...] = product(right).astype(BF16)
    remote(cright.at[bottom], from_left.at[bottom], rs_send.at[2], rs_recv.at[2], ep, right).start()
    cleft[...] = product(left).astype(BF16)
    remote(cleft.at[top], from_right.at[top], rs_send.at[3], rs_recv.at[3], ep, left).start()
    cown[...] = product(tp)

    arrived(down_pass.at[0], down_recv.at[2])
    remote(down_pass.at[0], down_rows(left, 0, half), down_send.at[4], down_recv.at[4], ep, right).start()
    arrived(down_pass.at[1], down_recv.at[3])
    remote(down_pass.at[1], down_rows(right, half, half), down_send.at[5], down_recv.at[5], ep, left).start()

    arrived(half_a, rs_recv.at[0])
    cright[top] = (cright[top].astype(F32) + half_a[...].astype(F32)).astype(BF16)
    remote(cright.at[top], from_left.at[top], rs_send.at[4], rs_recv.at[4], ep, right).start()
    arrived(half_b, rs_recv.at[1])
    cleft[bottom] = (cleft[bottom].astype(F32) + half_b[...].astype(F32)).astype(BF16)
    remote(cleft.at[bottom], from_right.at[bottom], rs_send.at[5], rs_recv.at[5], ep, left).start()

    def parts_of(count):
        cut = (count // 2 + 15) // 16 * 16
        return (0, cut), (cut, count - cut)

    def region(ref, lanes, first, rows, q):
        return ref.at[first : first + rows, lanes(q)]

    def gather_start(i, ref, lanes, first, count):
        own = region(ref, lanes, first, count, tp)
        remote(own, own, ag_send.at[i, 0], ag_recv.at[i, 0], ep, right).start()
        remote(own, own, ag_send.at[i, 1], ag_recv.at[i, 1], ep, left).start()

    def gather_pass(i, ref, lanes, first, count):
        (a, na), (b, nb) = parts_of(count)
        arrived(region(ref, lanes, first, count, left), ag_recv.at[i, 0])
        half = region(ref, lanes, first + a, na, left)
        remote(half, half, ag_send.at[i, 2], ag_recv.at[i, 2], ep, right).start()
        arrived(region(ref, lanes, first, count, right), ag_recv.at[i, 1])
        half = region(ref, lanes, first + b, nb, right)
        remote(half, half, ag_send.at[i, 3], ag_recv.at[i, 3], ep, left).start()

    def gather_end(i, ref, lanes, first, count):
        (a, na), (b, nb) = parts_of(count)
        arrived(region(ref, lanes, first + a, na, across), ag_recv.at[i, 2])
        arrived(region(ref, lanes, first + b, nb, across), ag_recv.at[i, 3])

    def gather_sent(i, ref, lanes, first, count):
        (a, na), (b, nb) = parts_of(count)
        left_here(region(ref, lanes, first, count, tp), ag_send.at[i, 0])
        left_here(region(ref, lanes, first, count, tp), ag_send.at[i, 1])
        left_here(region(ref, lanes, first + a, na, left), ag_send.at[i, 2])
        left_here(region(ref, lanes, first + b, nb, right), ag_send.at[i, 3])

    def of_batch(batch):
        first, count = BATCHES[batch]
        return first * ROWS, count * ROWS

    def rows_gather(step, batch):
        step(batch, xin, at_quarter, *of_batch(batch))

    def hidden_gather(step, batch):
        step(len(BATCHES) + batch, hid, at_ff, *of_batch(batch))

    def come(batch):
        first, count = BATCHES[batch]
        for group in range(first, first + count):
            start = group * ROWS
            if group < NEAR:
                main, rest = xin.at[start : start + BODY], in_near_rest.at[group]
            else:
                main, rest = xin.at[start : start + BODY, far_lanes()], in_far_rest.at[group - NEAR]
            sent_or_come(group, arrived, main, rest, go_recv, go_rest_recv)
            if group < NEAR:
                xin[start + BODY : start + ROWS, :] = unpack_rest(rest[...])
            else:
                xin[start + BODY : start + ROWS, far_lanes()] = unpack_rest(rest[...])

    def hidden(batch):
        first, count = of_batch(batch)
        rows = xin[first : first + count, :]
        value = silu(dot(rows, wg[...])) * dot(rows, wu[...])
        hid[first : first + count, at_ff(tp)] = value.astype(BF16)

    def send_back(batch):
        first, count = BATCHES[batch]
        start = first * ROWS
        rows = dot(hid[start : start + count * ROWS, :], down[...])
        for group in range(first, first + count):
            own = rows[(group - first) * ROWS : (group - first + 1) * ROWS]
            back_send[group] = own[0:BODY].astype(BF16)
            back_send_rest[group] = pack_rest(own[BODY:]).astype(BF16)
            exchange(
                group,
                -1,
                back_send.at[group],
                back.at[row_of(group, mine)],
                back_send_rest.at[group],
                back_rest.at[group, mine],
                back_ssem,
                back_rsem,
                back_rest_ssem,
                back_rest_rsem,
            )
            if group == 0:
                back[row_of(0, mine), :] = back_send[0, place_rows(mine), :]
                back_rest[0, mine] = back_send_rest[0, mine]

    wide = jnp.where(tall == 0, slot_first.astype(F32), jnp.where(tall == 1, slot_second.astype(F32), 0.0))
    given = weights_ref[...]
    wide = jnp.where(tall == 2, given[0:1, :], jnp.where(tall == 3, given[1:2, :], wide))
    turned = wide.T
    slot_one, slot_two = turned[:, 0:1].astype(jnp.int32), turned[:, 1:2].astype(jnp.int32)
    weight_one, weight_two = turned[:, 2:3], turned[:, 3:4]

    def combine(batch):
        first, count = BATCHES[batch]
        for group in range(first, first + count):
            start = group * ROWS
            sent_or_come(
                group, arrived, back.at[start : start + BODY], back_rest.at[group], back_rsem, back_rest_rsem
            )
            back[start + BODY : start + ROWS, :] = unpack_rest(back_rest[group])
        start = first * ROWS
        lane = iota((tokens, count * ROWS), 1) + start
        mix = jnp.where(lane == slot_one, weight_one, 0.0) + jnp.where(lane == slot_two, weight_two, 0.0)
        high = mix.astype(BF16)
        low = (mix - high.astype(F32)).astype(BF16)
        rows = back[start : start + count * ROWS, :]
        total[...] += dot(high, rows) + dot(low, rows)

    come(0)
    loads["wg"].wait()
    loads["wu"].wait()
    hidden(0)
    hidden_gather(gather_start, 0)
    come(1)
    rows_gather(gather_start, 1)
    hidden_gather(gather_pass, 0)
    come(2)
    rows_gather(gather_start, 2)
    rows_gather(gather_pass, 1)
    come(3)
    rows_gather(gather_start, 3)

    loads["down"].wait()
    arrived(down_rows(left, 0, ff), down_recv.at[0])
    arrived(down_rows(right, 0, ff), down_recv.at[1])
    arrived(down_rows(across, 0, half), down_recv.at[4])
    arrived(down_rows(across, half, half), down_recv.at[5])
    hidden_gather(gather_end, 0)
    send_back(0)

    rows_gather(gather_end, 1)
    hidden(1)
    hidden_gather(gather_start, 1)
    rows_gather(gather_pass, 2)
    rows_gather(gather_pass, 3)
    rows_gather(gather_end, 2)
    hidden(2)
    hidden_gather(gather_start, 2)
    hidden_gather(gather_pass, 1)
    hidden_gather(gather_end, 1)
    send_back(1)
    rows_gather(gather_end, 3)
    hidden(3)
    hidden_gather(gather_start, 3)
    hidden_gather(gather_pass, 2)
    hidden_gather(gather_end, 2)
    send_back(2)
    hidden_gather(gather_pass, 3)

    arrived(from_left.at[bottom], rs_recv.at[2])
    arrived(from_right.at[top], rs_recv.at[3])
    arrived(from_left.at[top], rs_recv.at[4])
    arrived(from_right.at[bottom], rs_recv.at[5])
    conv_out[...] = (cown[...] + from_left[...].astype(F32) + from_right[...].astype(F32)).astype(BF16)

    combine(0)
    hidden_gather(gather_end, 3)
    send_back(3)
    combine(1)
    combine(2)
    combine(3)
    moe_out[...] = total[...].astype(BF16)

    left_here(tail, halo_send)
    left_here(ed.at[:, at_quarter(right)], down_send.at[0])
    left_here(ed.at[:, at_quarter(left)], down_send.at[1])
    left_here(ed.at[0:half, at_quarter(across)], down_send.at[2])
    left_here(ed.at[half:ff, at_quarter(across)], down_send.at[3])
    left_here(down_pass.at[0], down_send.at[4])
    left_here(down_pass.at[1], down_send.at[5])
    for i in range(3):
        left_here(stat_send, stat_ssem.at[i])
    for i, part in enumerate((cfar.at[top], cfar.at[bottom], cright.at[bottom], cleft.at[top], cright.at[top], cleft.at[bottom])):
        left_here(part, rs_send.at[i])
    for group in range(len(ORDER)):
        if group < NEAR:
            main, rest = send_near.at[group], send_near_rest.at[group]
        else:
            main, rest = send_far.at[group - NEAR], send_far_rest.at[group - NEAR]
        sent_or_come(group, left_here, main, rest, go_send, go_rest_send)
        sent_or_come(group, left_here, back_send.at[group], back_send_rest.at[group], back_ssem, back_rest_ssem)
    for batch in range(len(BATCHES)):
        if batch > 0:
            rows_gather(gather_sent, batch)
        hidden_gather(gather_sent, batch)


def local(
    conv_value,
    conv_gate,
    conv_taps,
    conv_gain,
    conv_proj,
    moe_tokens,
    moe_gain,
    routes,
    route_weights,
    expert_gate,
    expert_up,
    expert_down,
    shared_gate,
    shared_up,
    shared_down,
):
    tokens, width = moe_tokens.shape
    quarter = conv_value.shape[1]
    ff = expert_gate.shape[2]
    full_ff = ff * lax.axis_size("tp")
    shared_ff = shared_gate.shape[1]
    groups = len(ORDER)
    far = groups - NEAR
    hbm = pl.BlockSpec(memory_space=pl.ANY)
    vmem = pl.BlockSpec(memory_space=pltpu.VMEM)
    dma = pltpu.SemaphoreType.DMA

    def buf(*shape):
        return pltpu.VMEM(shape, BF16)

    def wide(*shape):
        return pltpu.VMEM(shape, F32)

    scratch = [
        buf(tokens, quarter),
        buf(tokens, quarter),
        buf(quarter, width),
        buf(tokens, width),
        buf(width, ff),
        buf(width, ff),
        buf(width, shared_ff),
        buf(width, shared_ff),
        buf(shared_ff, quarter),
        buf(tokens, width),
        buf(NEAR, BODY, width),
        buf(NEAR, 8, 8, 512),
        buf(far, BODY, quarter),
        buf(far, 8, 8, 128),
        buf(groups * ROWS, width),
        buf(NEAR, 8, 8, 512),
        buf(far, 8, 8, 128),
        buf(groups * ROWS, full_ff),
        buf(full_ff, quarter),
        buf(2, ff // 2, quarter),
        buf(groups, BODY, quarter),
        buf(groups, 8, 8, 128),
        buf(groups * ROWS, quarter),
        buf(groups, 8, 8, 128),
        wide(tokens, quarter),
        wide(quarter // 128, tokens + 32, 128),
        wide(quarter // 128, 32, 128),
        wide(quarter // 128, tokens, 128),
        wide(tokens, 128),
        wide(tokens, 128),
        buf(32, quarter),
        buf(32, quarter),
        wide(8, tokens),
        wide(4, 8, tokens),
        buf(tokens, quarter),
        buf(tokens, quarter),
        buf(tokens, quarter),
        buf(tokens, quarter),
        wide(tokens, quarter),
        buf(tokens // 2, quarter),
        buf(tokens // 2, quarter),
        buf(tokens, quarter),
        buf(tokens, quarter),
        dma((10,)),
        dma((groups,)),
        dma((groups,)),
        dma((groups,)),
        dma((groups,)),
        dma((groups,)),
        dma((groups,)),
        dma((groups,)),
        dma((groups,)),
        dma((2 * len(BATCHES), 4)),
        dma((2 * len(BATCHES), 4)),
        dma((6,)),
        dma((6,)),
        dma,
        dma,
        dma((3,)),
        dma((3,)),
        dma((6,)),
        dma((6,)),
    ]
    result = jax.ShapeDtypeStruct((tokens, quarter), BF16)
    return pl.pallas_call(
        kernel,
        out_shape=(result, result),
        in_specs=[hbm, hbm, vmem, vmem, hbm, hbm, vmem, vmem, vmem, hbm, hbm, hbm, hbm, hbm, hbm],
        out_specs=(vmem, vmem),
        scratch_shapes=scratch,
        compiler_params=pltpu.CompilerParams(collective_id=0, has_side_effects=True),
    )(
        conv_value,
        conv_gate,
        conv_taps,
        conv_gain.reshape(1, -1),
        conv_proj,
        moe_tokens,
        moe_gain.reshape(1, -1),
        routes.T,
        route_weights.T,
        expert_gate,
        expert_up,
        expert_down,
        shared_gate,
        shared_up,
        shared_down,
    )


def solution(mesh):
    placed = (
        P("ep", "tp"),
        P("ep", "tp"),
        P(None, "tp"),
        P("tp"),
        P("tp", None),
        P("ep", None),
        P(),
        P("ep", None),
        P("ep", None),
        P("ep", None, "tp"),
        P("ep", None, "tp"),
        P("ep", "tp", None),
        P(),
        P(),
        P(None, "tp"),
    )
    return jax.shard_map(
        local, mesh=mesh, in_specs=placed, out_specs=(P("ep", "tp"), P("ep", "tp")), check_vma=False
    )
```

```python
import functools

import jax
import jax.numpy as jnp
from jax import lax
from jax.experimental import pallas as pl
from jax.experimental.pallas import tpu as pltpu
from jax.sharding import PartitionSpec as P

MESH = pl.DeviceIdType.MESH
F32 = jnp.float32
BF16 = jnp.bfloat16
epsilon = 1e-05

ORDER = (0, 1, 7, 2, 6, 3, 5, 4)
PLANE = 8
MAIN = 16
REST = 2
ROWS = PLANE * (MAIN + REST)
BODY = PLANE * MAIN
NEAR = 3
SENT = (6, 7, 4, 5, 3, 2, 0, 1)


def silu(v):
    return v / (1.0 + jnp.exp(-v))


def dot(a, b):
    return jnp.dot(a, b, preferred_element_type=F32)


def iota(shape, dim):
    return lax.broadcasted_iota(jnp.int32, shape, dim)


def kernel(
    cv_hbm,
    cg_hbm,
    taps_hbm,
    cgain_hbm,
    cproj_hbm,
    tok_hbm,
    mgain_hbm,
    routes_hbm,
    weights_hbm,
    eg_hbm,
    eu_hbm,
    ed_hbm,
    sg_hbm,
    su_hbm,
    sd_hbm,
    conv_out,
    moe_out,
    cv,
    cg,
    taps_ref,
    cgain_ref,
    mgain_ref,
    routes_ref,
    weights_ref,
    cproj,
    tok,
    wg,
    wu,
    sg,
    su,
    sd,
    norm,
    send_near,
    send_near_rest,
    send_far,
    send_far_rest,
    xin,
    in_near_rest,
    in_far_rest,
    hid,
    down,
    back_send,
    back_send_rest,
    back,
    back_rest,
    total,
    padded,
    taps,
    conv,
    ssum,
    ssq,
    tail,
    halo,
    stat_send,
    stat,
    act,
    cfar,
    cright,
    cleft,
    cown,
    half_a,
    half_b,
    from_left,
    from_right,
    load_sem,
    go_send,
    go_recv,
    go_rest_send,
    go_rest_recv,
    back_ssem,
    back_rsem,
    back_rest_ssem,
    back_rest_rsem,
    ag_send,
    ag_recv,
    down_send,
    down_recv,
    halo_send,
    halo_recv,
    stat_ssem,
    stat_rsem,
    rs_send,
    rs_recv,
):
    ep, tp = lax.axis_index("ep"), lax.axis_index("tp")
    n_ep, n_tp = lax.axis_size("ep"), lax.axis_size("tp")
    planes = n_ep // PLANE
    z, mine = ep // PLANE, lax.rem(ep, PLANE)
    right, left, across = (lax.rem(tp + i, n_tp) for i in (1, 3, 2))
    tokens, width = tok.shape
    quarter = width // n_tp
    ff = wg.shape[1]

    def remote(src, dst, ssem, rsem, to_ep, to_tp):
        return pltpu.make_async_remote_copy(
            src_ref=src,
            dst_ref=dst,
            send_sem=ssem,
            recv_sem=rsem,
            device_id=(to_ep, to_tp),
            device_id_type=MESH,
        )

    def arrived(ref, sem):
        remote(ref, ref, sem, sem, ep, right).wait_recv()

    def left_here(ref, sem):
        remote(ref, ref, sem, sem, ep, right).wait_send()

    barrier = pltpu.get_barrier_semaphore()

    @pl.loop(1, n_ep)
    def _(o):
        pl.semaphore_signal(
            barrier, inc=1, device_id=(lax.rem(ep + o, n_ep), tp), device_id_type=MESH
        )

    for peer in (right, left, across):
        pl.semaphore_signal(barrier, inc=1, device_id=(ep, peer), device_id_type=MESH)

    def at_quarter(q):
        return pl.ds(pl.multiple_of(q * quarter, quarter), quarter)

    def at_ff(q):
        return pl.ds(pl.multiple_of(q * ff, ff), ff)

    loads = {}
    for number, (name, src, dst) in enumerate(
        (
            ("tok", tok_hbm, tok),
            ("mgain", mgain_hbm, mgain_ref),
            ("routes", routes_hbm, routes_ref),
            ("cv", cv_hbm, cv),
            ("cg", cg_hbm, cg),
            ("taps", taps_hbm, taps_ref),
            ("cgain", cgain_hbm, cgain_ref),
            ("weights", weights_hbm, weights_ref),
            ("sg", sg_hbm, sg),
            ("su", su_hbm, su),
            ("sd", sd_hbm, sd),
            ("cproj", cproj_hbm, cproj),
            ("wg", eg_hbm.at[0], wg),
            ("wu", eu_hbm.at[0], wu),
            ("down", ed_hbm.at[0, :, at_quarter(tp)], down.at[at_ff(tp)]),
        )
    ):
        loads[name] = pltpu.make_async_copy(src, dst, load_sem.at[number])
        loads[name].start()

    loads["tok"].wait()
    loads["mgain"].wait()
    for r in range(0, tokens, 64):
        rows = tok[r : r + 64, :].astype(F32)
        mean = jnp.sum(rows, axis=1, keepdims=True) * (1.0 / width)
        centered = rows - mean
        var = jnp.sum(centered * centered, axis=1, keepdims=True) * (1.0 / width)
        norm[r : r + 64, :] = (centered * lax.rsqrt(var + epsilon) * mgain_ref[...]).astype(BF16)

    loads["routes"].wait()
    routes = routes_ref[...]
    first, second = routes[0:1, :], routes[1:2, :]
    names = iota((n_ep, tokens), 0)
    is_first = (names == first).astype(F32)
    is_second = (names == second).astype(F32)
    earlier = (iota((tokens, tokens), 0) < iota((tokens, tokens), 1)).astype(F32).astype(BF16)
    before = dot((is_first + is_second).astype(BF16), earlier)

    def slot_of(route, chosen):
        rank = jnp.sum(before * chosen, axis=0, keepdims=True).astype(jnp.int32)
        away = ((route >> 3) - z + planes) & (planes - 1)
        place = route & (PLANE - 1)
        group = jnp.where(away == 0, 0, jnp.where(away <= 4, 2 * away - 1, 2 * (planes - away)))
        inside = jnp.where(rank < MAIN, place * MAIN + rank, BODY + place * REST + rank - MAIN)
        return group * ROWS + inside

    slot_first, slot_second = slot_of(first, is_first), slot_of(second, is_second)

    way = iota((64, 64), 0)
    here = iota((64, 64), 1)
    same = (way >> 3 == (here >> 1 & 7)) & ((way >> 1 & 3) == here >> 4) & ((way & 1) == (here & 1))
    to_way = same.astype(F32).astype(BF16)
    way = iota((64, 64), 1)
    here = iota((64, 64), 0)
    same = (way >> 3 == (here >> 1 & 7)) & ((way >> 1 & 3) == here >> 4) & ((way & 1) == (here & 1))
    to_here = same.astype(F32).astype(BF16)

    def pack_rest(rest):
        n = rest.shape[1] // 512
        stacked = jnp.concatenate(
            [
                jnp.concatenate(
                    [rest[:, q * 512 + g * 128 : q * 512 + (g + 1) * 128] for q in range(n)], axis=1
                )
                for g in range(4)
            ],
            axis=0,
        )
        return dot(to_way, stacked.astype(BF16)).reshape(8, 8, n * 128)

    def unpack_rest(packed):
        n = packed.shape[2] // 128
        stacked = dot(to_here, packed.astype(F32).reshape(64, n * 128).astype(BF16))
        return jnp.concatenate(
            [
                stacked[g * 16 : (g + 1) * 16, q * 128 : (q + 1) * 128]
                for q in range(n)
                for g in range(4)
            ],
            axis=1,
        ).astype(BF16)

    def row_of(group, place, count=MAIN):
        return pl.ds(pl.multiple_of(group * ROWS + place * MAIN, MAIN), count)

    def place_rows(place):
        return pl.ds(pl.multiple_of(place * MAIN, MAIN), MAIN)

    def exchange(group, sign, main, main_at, rest, rest_at, ssem, rsem, rest_ssem, rest_rsem):
        plane = lax.rem(z + sign * ORDER[group] + planes, planes)

        @pl.loop(1 if group == 0 else 0, PLANE)
        def _(o):
            place = lax.rem(mine + o, PLANE)
            to = plane * PLANE + place
            remote(main.at[place_rows(place)], main_at, ssem.at[group], rsem.at[group], to, tp).start()
            remote(rest.at[place], rest_at, rest_ssem.at[group], rest_rsem.at[group], to, tp).start()

    def sent_or_come(group, wait, main, rest, sem, rest_sem):
        count = PLANE - 1 if group == 0 else PLANE
        wait(main.at[0 : count * MAIN], sem.at[group])
        wait(rest.at[0:count], rest_sem.at[group])

    def far_lanes():
        return at_quarter(tp)

    loads["cv"].wait()
    loads["cg"].wait()
    loads["taps"].wait()
    blocks = quarter // 128
    extra = halo.shape[0]
    for b in range(blocks):
        lanes = slice(b * 128, (b + 1) * 128)
        gated = (cv[:, lanes].astype(F32) * jax.nn.sigmoid(cg[:, lanes].astype(F32))).astype(BF16)
        padded[b, extra:, :] = gated.astype(F32)
        tail[:, lanes] = gated[tokens - extra :]
        taps[b, 0:31] = taps_ref[:, lanes].astype(F32)

    pl.semaphore_wait(barrier, n_ep - 1 + n_tp - 1)

    next_ep = lax.rem(ep + 1, n_ep)
    remote(tail, halo, halo_send, halo_recv, next_ep, tp).start()

    def down_rows(owner):
        return down.at[at_ff(owner)]

    ed = ed_hbm.at[0]
    remote(ed.at[:, at_quarter(right)], down_rows(tp), down_send.at[0], down_recv.at[0], ep, right).start()
    remote(ed.at[:, at_quarter(left)], down_rows(tp), down_send.at[1], down_recv.at[1], ep, left).start()

    for group in SENT:
        row = iota((ROWS, tokens), 0) + group * ROWS
        pick = ((row == slot_first) | (row == slot_second)).astype(F32).astype(BF16)
        if group < NEAR:
            rows = dot(pick, norm[...])
            send_near[group] = rows[0:BODY].astype(BF16)
            send_near_rest[group] = pack_rest(rows[BODY:]).astype(BF16)
            main, rest = send_near.at[group], send_near_rest.at[group]
            main_at, rest_at = xin.at[row_of(group, mine)], in_near_rest.at[group, mine]
        else:
            rows = dot(pick, norm[:, far_lanes()])
            send_far[group - NEAR] = rows[0:BODY].astype(BF16)
            send_far_rest[group - NEAR] = pack_rest(rows[BODY:]).astype(BF16)
            main, rest = send_far.at[group - NEAR], send_far_rest.at[group - NEAR]
            main_at = xin.at[row_of(group, mine), far_lanes()]
            rest_at = in_far_rest.at[group - NEAR, mine]
        exchange(group, 1, main, main_at, rest, rest_at, go_send, go_recv, go_rest_send, go_rest_recv)
        if group == 0:
            xin[row_of(0, mine), :] = send_near[0, place_rows(mine), :]
            in_near_rest[0, mine] = send_near_rest[0, mine]

    def parts_of(count):
        cut = (count // 2 + 15) // 16 * 16
        return (0, cut), (cut, count - cut)

    def region(ref, lanes, first, rows, q):
        return ref.at[first : first + rows, lanes(q)]

    def gather_start(i, ref, lanes, first, count):
        own = region(ref, lanes, first, count, tp)
        remote(own, own, ag_send.at[i, 0], ag_recv.at[i, 0], ep, right).start()
        remote(own, own, ag_send.at[i, 1], ag_recv.at[i, 1], ep, left).start()

    def gather_pass(i, ref, lanes, first, count):
        (a, na), (b, nb) = parts_of(count)
        arrived(region(ref, lanes, first, count, left), ag_recv.at[i, 0])
        half = region(ref, lanes, first + a, na, left)
        remote(half, half, ag_send.at[i, 2], ag_recv.at[i, 2], ep, right).start()
        arrived(region(ref, lanes, first, count, right), ag_recv.at[i, 1])
        half = region(ref, lanes, first + b, nb, right)
        remote(half, half, ag_send.at[i, 3], ag_recv.at[i, 3], ep, left).start()

    def gather_end(i, ref, lanes, first, count):
        (a, na), (b, nb) = parts_of(count)
        arrived(region(ref, lanes, first + a, na, across), ag_recv.at[i, 2])
        arrived(region(ref, lanes, first + b, nb, across), ag_recv.at[i, 3])

    def gather_sent(i, ref, lanes, first, count):
        (a, na), (b, nb) = parts_of(count)
        left_here(region(ref, lanes, first, count, tp), ag_send.at[i, 0])
        left_here(region(ref, lanes, first, count, tp), ag_send.at[i, 1])
        left_here(region(ref, lanes, first + a, na, left), ag_send.at[i, 2])
        left_here(region(ref, lanes, first + b, nb, right), ag_send.at[i, 3])

    def rows_gather(step, group):
        step(group, xin, at_quarter, group * ROWS, ROWS)

    def hidden_gather(step, group):
        step(len(ORDER) + group, hid, at_ff, group * ROWS, ROWS)

    def come(group):
        start = group * ROWS
        if group < NEAR:
            main, rest = xin.at[start : start + BODY], in_near_rest.at[group]
        else:
            main, rest = xin.at[start : start + BODY, far_lanes()], in_far_rest.at[group - NEAR]
        sent_or_come(group, arrived, main, rest, go_recv, go_rest_recv)
        if group < NEAR:
            xin[start + BODY : start + ROWS, :] = unpack_rest(rest[...])
        else:
            xin[start + BODY : start + ROWS, far_lanes()] = unpack_rest(rest[...])

    def hidden(group):
        start = group * ROWS
        rows = xin[start : start + ROWS, :]
        value = silu(dot(rows, wg[...])) * dot(rows, wu[...])
        hid[start : start + ROWS, at_ff(tp)] = value.astype(BF16)

    def send_back(group):
        start = group * ROWS
        own = dot(hid[start : start + ROWS, :], down[...])
        back_send[group] = own[0:BODY].astype(BF16)
        back_send_rest[group] = pack_rest(own[BODY:]).astype(BF16)
        exchange(
            group,
            -1,
            back_send.at[group],
            back.at[row_of(group, mine)],
            back_send_rest.at[group],
            back_rest.at[group, mine],
            back_ssem,
            back_rsem,
            back_rest_ssem,
            back_rest_rsem,
        )
        if group == 0:
            back[row_of(0, mine), :] = back_send[0, place_rows(mine), :]
            back_rest[0, mine] = back_send_rest[0, mine]

    tall = iota((128, tokens), 0)
    wide = jnp.where(tall == 0, slot_first.astype(F32), jnp.where(tall == 1, slot_second.astype(F32), 0.0))
    loads["weights"].wait()
    given = weights_ref[...]
    wide = jnp.where(tall == 2, given[0:1, :], jnp.where(tall == 3, given[1:2, :], wide))
    turned = wide.T
    slot_one, slot_two = turned[:, 0:1].astype(jnp.int32), turned[:, 1:2].astype(jnp.int32)
    weight_one, weight_two = turned[:, 2:3], turned[:, 3:4]

    def combine(group):
        start = group * ROWS
        sent_or_come(
            group, arrived, back.at[start : start + BODY], back_rest.at[group], back_rsem, back_rest_rsem
        )
        back[start + BODY : start + ROWS, :] = unpack_rest(back_rest[group])
        lane = iota((tokens, ROWS), 1) + start
        mix = jnp.where(lane == slot_one, weight_one, 0.0) + jnp.where(lane == slot_two, weight_two, 0.0)
        high = mix.astype(BF16)
        low = (mix - high.astype(F32)).astype(BF16)
        rows = back[start : start + ROWS, :]
        total[...] += dot(high, rows) + dot(low, rows)

    arrived(halo, halo_recv)
    for b in range(blocks):
        before_rows = halo[:, b * 128 : (b + 1) * 128].astype(F32)
        padded[b, 0:extra, :] = jnp.where(ep == 0, jnp.zeros_like(before_rows), before_rows)
    ssum[...] = jnp.zeros_like(ssum)
    ssq[...] = jnp.zeros_like(ssq)

    @pl.loop(0, blocks)
    def _(b):
        for r in range(0, tokens, 64):
            acc = jnp.zeros((64, 128), F32)
            for offset in range(31):
                start = r + offset + extra - 30
                acc = acc + taps[b, offset : offset + 1, :] * padded[b, start : start + 64, :]
            conv[b, r : r + 64, :] = acc
            ssum[r : r + 64, :] += acc
            ssq[r : r + 64, :] += acc * acc

    eighth = iota((8, tokens), 0)
    sums = jnp.sum(ssum[...].T, axis=0, keepdims=True)
    squares = jnp.sum(ssq[...].T, axis=0, keepdims=True)
    own_stat = jnp.where(eighth == 0, sums, jnp.where(eighth == 1, squares, 0.0))
    stat_send[...] = own_stat
    stat[tp] = own_stat
    for i, peer in enumerate((right, left, across)):
        remote(stat_send, stat.at[tp], stat_ssem.at[i], stat_rsem.at[i], ep, peer).start()

    remote(ed.at[:, at_quarter(across)], down_rows(tp), down_send.at[2], down_recv.at[2], ep, across).start()

    loads["sg"].wait()
    loads["su"].wait()
    loads["sd"].wait()
    shared = (silu(dot(norm[...], sg[...])) * dot(norm[...], su[...])).astype(BF16)
    total[...] = dot(shared, sd[...])

    come(6)
    rows_gather(gather_start, 6)
    for i, peer in enumerate((left, right, across)):
        arrived(stat.at[peer], stat_rsem.at[i])
    sums = stat[0] + stat[1] + stat[2] + stat[3]
    average = sums[0:1] * (1.0 / width)
    variance = sums[1:2] * (1.0 / width) - average * average
    scale = lax.rsqrt(variance + epsilon)
    turned = jnp.where(tall == 0, average, jnp.where(tall == 1, scale, 0.0)).T
    average, scale = turned[:, 0:1], turned[:, 1:2]
    loads["cgain"].wait()
    for b in range(blocks):
        lanes = slice(b * 128, (b + 1) * 128)
        act[:, lanes] = silu((conv[b] - average) * scale * cgain_ref[:, lanes]).astype(BF16)

    loads["cproj"].wait()
    upper = tokens // 2
    top, bottom = slice(0, upper), slice(upper, tokens)

    def product(q):
        return dot(act[...], cproj[:, at_quarter(q)])

    cfar[...] = product(across).astype(BF16)
    cright[...] = product(right).astype(BF16)
    cleft[...] = product(left).astype(BF16)
    cown[...] = product(tp)

    remote(cfar.at[top], half_a, rs_send.at[0], rs_recv.at[0], ep, right).start()
    remote(cfar.at[bottom], half_b, rs_send.at[1], rs_recv.at[1], ep, left).start()
    remote(cright.at[bottom], from_left.at[bottom], rs_send.at[2], rs_recv.at[2], ep, right).start()
    remote(cleft.at[top], from_right.at[top], rs_send.at[3], rs_recv.at[3], ep, left).start()

    come(7)
    rows_gather(gather_start, 7)
    rows_gather(gather_pass, 6)
    come(4)
    rows_gather(gather_start, 4)
    rows_gather(gather_pass, 7)
    rows_gather(gather_end, 6)
    loads["wg"].wait()
    loads["wu"].wait()
    hidden(6)
    hidden_gather(gather_start, 6)
    rows_gather(gather_pass, 4)
    come(5)
    rows_gather(gather_start, 5)
    rows_gather(gather_end, 7)
    hidden(7)
    hidden_gather(gather_start, 7)
    hidden_gather(gather_pass, 6)
    rows_gather(gather_pass, 5)
    come(3)
    rows_gather(gather_start, 3)
    rows_gather(gather_end, 4)
    hidden(4)
    hidden_gather(gather_start, 4)
    hidden_gather(gather_pass, 7)
    loads["down"].wait()
    arrived(down_rows(left), down_recv.at[0])
    arrived(down_rows(right), down_recv.at[1])
    arrived(down_rows(across), down_recv.at[2])
    hidden_gather(gather_end, 6)
    send_back(6)
    rows_gather(gather_pass, 3)
    hidden_gather(gather_pass, 4)
    rows_gather(gather_end, 5)
    hidden(5)
    hidden_gather(gather_start, 5)
    hidden_gather(gather_end, 7)
    send_back(7)
    rows_gather(gather_end, 3)
    hidden(3)
    hidden_gather(gather_start, 3)
    hidden_gather(gather_end, 4)
    send_back(4)
    hidden_gather(gather_pass, 5)
    come(0)
    hidden(0)
    hidden_gather(gather_start, 0)
    come(2)
    hidden(2)
    hidden_gather(gather_start, 2)
    hidden_gather(gather_pass, 3)
    hidden_gather(gather_end, 5)
    send_back(5)
    arrived(half_a, rs_recv.at[0])
    cright[top] = (cright[top].astype(F32) + half_a[...].astype(F32)).astype(BF16)
    remote(cright.at[top], from_left.at[top], rs_send.at[4], rs_recv.at[4], ep, right).start()
    arrived(half_b, rs_recv.at[1])
    cleft[bottom] = (cleft[bottom].astype(F32) + half_b[...].astype(F32)).astype(BF16)
    remote(cleft.at[bottom], from_right.at[bottom], rs_send.at[5], rs_recv.at[5], ep, left).start()

    come(1)
    hidden(1)
    hidden_gather(gather_start, 1)
    hidden_gather(gather_end, 3)
    send_back(3)
    hidden_gather(gather_pass, 0)
    hidden_gather(gather_pass, 2)
    hidden_gather(gather_end, 0)
    send_back(0)
    hidden_gather(gather_end, 2)
    send_back(2)
    hidden_gather(gather_pass, 1)
    combine(6)
    combine(7)
    hidden_gather(gather_end, 1)
    send_back(1)
    combine(4)
    combine(5)
    combine(3)
    arrived(from_left.at[bottom], rs_recv.at[2])
    arrived(from_right.at[top], rs_recv.at[3])
    arrived(from_left.at[top], rs_recv.at[4])
    arrived(from_right.at[bottom], rs_recv.at[5])
    conv_out[...] = (cown[...] + from_left[...].astype(F32) + from_right[...].astype(F32)).astype(BF16)

    combine(0)
    combine(2)
    combine(1)
    moe_out[...] = total[...].astype(BF16)
    left_here(tail, halo_send)
    left_here(ed.at[:, at_quarter(right)], down_send.at[0])
    left_here(ed.at[:, at_quarter(left)], down_send.at[1])
    left_here(ed.at[:, at_quarter(across)], down_send.at[2])
    for i in range(3):
        left_here(stat_send, stat_ssem.at[i])
    for i, part in enumerate((cfar.at[top], cfar.at[bottom], cright.at[bottom], cleft.at[top], cright.at[top], cleft.at[bottom])):
        left_here(part, rs_send.at[i])
    for group in range(len(ORDER)):
        if group < NEAR:
            main, rest = send_near.at[group], send_near_rest.at[group]
        else:
            main, rest = send_far.at[group - NEAR], send_far_rest.at[group - NEAR]
        sent_or_come(group, left_here, main, rest, go_send, go_rest_send)
        sent_or_come(group, left_here, back_send.at[group], back_send_rest.at[group], back_ssem, back_rest_ssem)
        if group >= NEAR:
            rows_gather(gather_sent, group)
        hidden_gather(gather_sent, group)


def handed_on(a_ref, b_ref, a_out, b_out):
    a_out[...] = a_ref[...]
    b_out[...] = b_ref[...]


def local(
    conv_value,
    conv_gate,
    conv_taps,
    conv_gain,
    conv_proj,
    moe_tokens,
    moe_gain,
    routes,
    route_weights,
    expert_gate,
    expert_up,
    expert_down,
    shared_gate,
    shared_up,
    shared_down,
):
    tokens, width = moe_tokens.shape
    quarter = conv_value.shape[1]
    ff = expert_gate.shape[2]
    full_ff = ff * lax.axis_size("tp")
    shared_ff = shared_gate.shape[1]
    groups = len(ORDER)
    far = groups - NEAR
    hbm = pl.BlockSpec(memory_space=pl.ANY)
    vmem = pl.BlockSpec(memory_space=pltpu.VMEM)
    dma = pltpu.SemaphoreType.DMA

    def buf(*shape):
        return pltpu.VMEM(shape, BF16)

    def wide(*shape):
        return pltpu.VMEM(shape, F32)

    scratch = [
        buf(tokens, quarter),
        buf(tokens, quarter),
        buf(31, quarter),
        wide(1, quarter),
        wide(1, width),
        pltpu.VMEM((2, tokens), jnp.int32),
        wide(2, tokens),
        buf(quarter, width),
        buf(tokens, width),
        buf(width, ff),
        buf(width, ff),
        buf(width, shared_ff),
        buf(width, shared_ff),
        buf(shared_ff, quarter),
        buf(tokens, width),
        buf(NEAR, BODY, width),
        buf(NEAR, 8, 8, 512),
        buf(far, BODY, quarter),
        buf(far, 8, 8, 128),
        buf(groups * ROWS, width),
        buf(NEAR, 8, 8, 512),
        buf(far, 8, 8, 128),
        buf(groups * ROWS, full_ff),
        buf(full_ff, quarter),
        buf(groups, BODY, quarter),
        buf(groups, 8, 8, 128),
        buf(groups * ROWS, quarter),
        buf(groups, 8, 8, 128),
        wide(tokens, quarter),
        wide(quarter // 128, tokens + 32, 128),
        wide(quarter // 128, 32, 128),
        wide(quarter // 128, tokens, 128),
        wide(tokens, 128),
        wide(tokens, 128),
        buf(32, quarter),
        buf(32, quarter),
        wide(8, tokens),
        wide(4, 8, tokens),
        buf(tokens, quarter),
        buf(tokens, quarter),
        buf(tokens, quarter),
        buf(tokens, quarter),
        wide(tokens, quarter),
        buf(tokens // 2, quarter),
        buf(tokens // 2, quarter),
        buf(tokens, quarter),
        buf(tokens, quarter),
        dma((15,)),
        dma((groups,)),
        dma((groups,)),
        dma((groups,)),
        dma((groups,)),
        dma((groups,)),
        dma((groups,)),
        dma((groups,)),
        dma((groups,)),
        dma((2 * groups, 4)),
        dma((2 * groups, 4)),
        dma((3,)),
        dma((3,)),
        dma,
        dma,
        dma((3,)),
        dma((3,)),
        dma((6,)),
        dma((6,)),
    ]
    result = jax.ShapeDtypeStruct((tokens, quarter), BF16)
    results = pl.pallas_call(
        kernel,
        out_shape=(result, result),
        in_specs=[hbm] * 15,
        out_specs=(vmem, vmem),
        scratch_shapes=scratch,
        compiler_params=pltpu.CompilerParams(collective_id=0, has_side_effects=True),
    )(
        conv_value,
        conv_gate,
        conv_taps,
        conv_gain.reshape(1, -1),
        conv_proj,
        moe_tokens,
        moe_gain.reshape(1, -1),
        routes.T,
        route_weights.T,
        expert_gate,
        expert_up,
        expert_down,
        shared_gate,
        shared_up,
        shared_down,
    )
    return pl.pallas_call(
        handed_on, out_shape=(result, result), in_specs=[vmem, vmem], out_specs=(vmem, vmem)
    )(*results)


def solution(mesh):
    placed = (
        P("ep", "tp"),
        P("ep", "tp"),
        P(None, "tp"),
        P("tp"),
        P("tp", None),
        P("ep", None),
        P(),
        P("ep", None),
        P("ep", None),
        P("ep", None, "tp"),
        P("ep", None, "tp"),
        P("ep", "tp", None),
        P(),
        P(),
        P(None, "tp"),
    )
    return jax.shard_map(
        local, mesh=mesh, in_specs=placed, out_specs=(P("ep", "tp"), P("ep", "tp")), check_vma=False
    )
```

```python
import functools

import jax
import jax.numpy as jnp
from jax import lax
from jax.experimental import pallas as pl
from jax.experimental.pallas import tpu as pltpu
from jax.sharding import PartitionSpec as P

MESH = pl.DeviceIdType.MESH
F32 = jnp.float32
BF16 = jnp.bfloat16
epsilon = 1e-05

ORDER = (0, 1, 7, 2, 6, 3, 5, 4)
PLANE = 8
MAIN = 16
REST = 2
ROWS = PLANE * (MAIN + REST)
BODY = PLANE * MAIN
NEAR = 3
SENT = (7, 5, 6, 3, 4, 2, 1, 0)


def silu(v):
    return v / (1.0 + jnp.exp(-v))


def dot(a, b):
    return jnp.dot(a, b, preferred_element_type=F32)


def iota(shape, dim):
    return lax.broadcasted_iota(jnp.int32, shape, dim)


def kernel(
    cv_hbm,
    cg_hbm,
    taps_hbm,
    cgain_hbm,
    cproj_hbm,
    tok_hbm,
    mgain_hbm,
    routes_hbm,
    weights_hbm,
    eg_hbm,
    eu_hbm,
    ed_hbm,
    sg_hbm,
    su_hbm,
    sd_hbm,
    conv_out,
    moe_out,
    cv,
    cg,
    taps_ref,
    cgain_ref,
    mgain_ref,
    routes_ref,
    weights_ref,
    cproj,
    tok,
    wg,
    wu,
    sg,
    su,
    sd,
    norm,
    send_near,
    send_near_rest,
    send_far,
    send_far_rest,
    xin,
    in_near_rest,
    in_far_rest,
    hid,
    down,
    back_send,
    back_send_rest,
    back,
    back_rest,
    total,
    padded,
    taps,
    conv,
    ssum,
    ssq,
    tail,
    halo,
    stat_send,
    stat,
    act,
    cfar,
    cright,
    cleft,
    cown,
    half_a,
    half_b,
    from_left,
    from_right,
    load_sem,
    go_send,
    go_recv,
    go_rest_send,
    go_rest_recv,
    back_ssem,
    back_rsem,
    back_rest_ssem,
    back_rest_rsem,
    ag_send,
    ag_recv,
    down_send,
    down_recv,
    halo_send,
    halo_recv,
    stat_ssem,
    stat_rsem,
    rs_send,
    rs_recv,
):
    ep, tp = lax.axis_index("ep"), lax.axis_index("tp")
    n_ep, n_tp = lax.axis_size("ep"), lax.axis_size("tp")
    planes = n_ep // PLANE
    z, mine = ep // PLANE, lax.rem(ep, PLANE)
    right, left, across = (lax.rem(tp + i, n_tp) for i in (1, 3, 2))
    tokens, width = tok.shape
    quarter = width // n_tp
    ff = wg.shape[1]

    def remote(src, dst, ssem, rsem, to_ep, to_tp):
        return pltpu.make_async_remote_copy(
            src_ref=src,
            dst_ref=dst,
            send_sem=ssem,
            recv_sem=rsem,
            device_id=(to_ep, to_tp),
            device_id_type=MESH,
        )

    def arrived(ref, sem):
        remote(ref, ref, sem, sem, ep, right).wait_recv()

    def left_here(ref, sem):
        remote(ref, ref, sem, sem, ep, right).wait_send()

    barrier = pltpu.get_barrier_semaphore()

    @pl.loop(1, n_ep)
    def _(o):
        pl.semaphore_signal(
            barrier, inc=1, device_id=(lax.rem(ep + o, n_ep), tp), device_id_type=MESH
        )

    for peer in (right, left, across):
        pl.semaphore_signal(barrier, inc=1, device_id=(ep, peer), device_id_type=MESH)

    def at_quarter(q):
        return pl.ds(pl.multiple_of(q * quarter, quarter), quarter)

    def at_ff(q):
        return pl.ds(pl.multiple_of(q * ff, ff), ff)

    loads = {}
    for number, (name, src, dst) in enumerate(
        (
            ("tok", tok_hbm, tok),
            ("mgain", mgain_hbm, mgain_ref),
            ("routes", routes_hbm, routes_ref),
            ("cv", cv_hbm, cv),
            ("cg", cg_hbm, cg),
            ("taps", taps_hbm, taps_ref),
            ("cgain", cgain_hbm, cgain_ref),
            ("weights", weights_hbm, weights_ref),
            ("sg", sg_hbm, sg),
            ("su", su_hbm, su),
            ("sd", sd_hbm, sd),
            ("cproj", cproj_hbm, cproj),
            ("wg", eg_hbm.at[0], wg),
            ("wu", eu_hbm.at[0], wu),
            ("down", ed_hbm.at[0, :, at_quarter(tp)], down.at[at_ff(tp)]),
        )
    ):
        loads[name] = pltpu.make_async_copy(src, dst, load_sem.at[number])
        loads[name].start()

    loads["tok"].wait()
    loads["mgain"].wait()
    for r in range(0, tokens, 64):
        rows = tok[r : r + 64, :].astype(F32)
        mean = jnp.sum(rows, axis=1, keepdims=True) * (1.0 / width)
        centered = rows - mean
        var = jnp.sum(centered * centered, axis=1, keepdims=True) * (1.0 / width)
        norm[r : r + 64, :] = (centered * lax.rsqrt(var + epsilon) * mgain_ref[...]).astype(BF16)

    loads["routes"].wait()
    routes = routes_ref[...]
    first, second = routes[0:1, :], routes[1:2, :]
    names = iota((n_ep, tokens), 0)
    is_first = (names == first).astype(F32)
    is_second = (names == second).astype(F32)
    earlier = (iota((tokens, tokens), 0) < iota((tokens, tokens), 1)).astype(F32).astype(BF16)
    before = dot((is_first + is_second).astype(BF16), earlier)

    def slot_of(route, chosen):
        rank = jnp.sum(before * chosen, axis=0, keepdims=True).astype(jnp.int32)
        away = ((route >> 3) - z + planes) & (planes - 1)
        place = route & (PLANE - 1)
        group = jnp.where(away == 0, 0, jnp.where(away <= 4, 2 * away - 1, 2 * (planes - away)))
        inside = jnp.where(rank < MAIN, place * MAIN + rank, BODY + place * REST + rank - MAIN)
        return group * ROWS + inside

    slot_first, slot_second = slot_of(first, is_first), slot_of(second, is_second)

    way = iota((64, 64), 0)
    here = iota((64, 64), 1)
    same = (way >> 3 == (here >> 1 & 7)) & ((way >> 1 & 3) == here >> 4) & ((way & 1) == (here & 1))
    to_way = same.astype(F32).astype(BF16)
    way = iota((64, 64), 1)
    here = iota((64, 64), 0)
    same = (way >> 3 == (here >> 1 & 7)) & ((way >> 1 & 3) == here >> 4) & ((way & 1) == (here & 1))
    to_here = same.astype(F32).astype(BF16)

    def pack_rest(rest):
        n = rest.shape[1] // 512
        stacked = jnp.concatenate(
            [
                jnp.concatenate(
                    [rest[:, q * 512 + g * 128 : q * 512 + (g + 1) * 128] for q in range(n)], axis=1
                )
                for g in range(4)
            ],
            axis=0,
        )
        return dot(to_way, stacked.astype(BF16)).reshape(8, 8, n * 128)

    def unpack_rest(packed):
        n = packed.shape[2] // 128
        stacked = dot(to_here, packed.astype(F32).reshape(64, n * 128).astype(BF16))
        return jnp.concatenate(
            [
                stacked[g * 16 : (g + 1) * 16, q * 128 : (q + 1) * 128]
                for q in range(n)
                for g in range(4)
            ],
            axis=1,
        ).astype(BF16)

    def row_of(group, place, count=MAIN):
        return pl.ds(pl.multiple_of(group * ROWS + place * MAIN, MAIN), count)

    def place_rows(place):
        return pl.ds(pl.multiple_of(place * MAIN, MAIN), MAIN)

    def exchange(group, sign, main, main_at, rest, rest_at, ssem, rsem, rest_ssem, rest_rsem):
        plane = lax.rem(z + sign * ORDER[group] + planes, planes)

        @pl.loop(1 if group == 0 else 0, PLANE)
        def _(o):
            place = lax.rem(mine + o, PLANE)
            to = plane * PLANE + place
            remote(main.at[place_rows(place)], main_at, ssem.at[group], rsem.at[group], to, tp).start()
            remote(rest.at[place], rest_at, rest_ssem.at[group], rest_rsem.at[group], to, tp).start()

    def sent_or_come(group, wait, main, rest, sem, rest_sem):
        count = PLANE - 1 if group == 0 else PLANE
        wait(main.at[0 : count * MAIN], sem.at[group])
        wait(rest.at[0:count], rest_sem.at[group])

    def far_lanes():
        return at_quarter(tp)

    loads["cv"].wait()
    loads["cg"].wait()
    loads["taps"].wait()
    blocks = quarter // 128
    extra = halo.shape[0]
    for b in range(blocks):
        lanes = slice(b * 128, (b + 1) * 128)
        gated = (cv[:, lanes].astype(F32) * jax.nn.sigmoid(cg[:, lanes].astype(F32))).astype(BF16)
        padded[b, extra:, :] = gated.astype(F32)
        tail[:, lanes] = gated[tokens - extra :]
        taps[b, 0:31] = taps_ref[:, lanes].astype(F32)

    pl.semaphore_wait(barrier, n_ep - 1 + n_tp - 1)

    next_ep = lax.rem(ep + 1, n_ep)
    remote(tail, halo, halo_send, halo_recv, next_ep, tp).start()

    def down_rows(owner):
        return down.at[at_ff(owner)]

    ed = ed_hbm.at[0]
    remote(ed.at[:, at_quarter(right)], down_rows(tp), down_send.at[0], down_recv.at[0], ep, right).start()
    remote(ed.at[:, at_quarter(left)], down_rows(tp), down_send.at[1], down_recv.at[1], ep, left).start()

    for group in SENT:
        row = iota((ROWS, tokens), 0) + group * ROWS
        pick = ((row == slot_first) | (row == slot_second)).astype(F32).astype(BF16)
        if group < NEAR:
            rows = dot(pick, norm[...])
            send_near[group] = rows[0:BODY].astype(BF16)
            send_near_rest[group] = pack_rest(rows[BODY:]).astype(BF16)
            main, rest = send_near.at[group], send_near_rest.at[group]
            main_at, rest_at = xin.at[row_of(group, mine)], in_near_rest.at[group, mine]
        else:
            rows = dot(pick, norm[:, far_lanes()])
            send_far[group - NEAR] = rows[0:BODY].astype(BF16)
            send_far_rest[group - NEAR] = pack_rest(rows[BODY:]).astype(BF16)
            main, rest = send_far.at[group - NEAR], send_far_rest.at[group - NEAR]
            main_at = xin.at[row_of(group, mine), far_lanes()]
            rest_at = in_far_rest.at[group - NEAR, mine]
        exchange(group, 1, main, main_at, rest, rest_at, go_send, go_recv, go_rest_send, go_rest_recv)
        if group == 0:
            xin[row_of(0, mine), :] = send_near[0, place_rows(mine), :]
            in_near_rest[0, mine] = send_near_rest[0, mine]

    def parts_of(count):
        cut = (count // 2 + 15) // 16 * 16
        return (0, cut), (cut, count - cut)

    def region(ref, lanes, first, rows, q):
        return ref.at[first : first + rows, lanes(q)]

    def gather_start(i, ref, lanes, first, count):
        own = region(ref, lanes, first, count, tp)
        remote(own, own, ag_send.at[i, 0], ag_recv.at[i, 0], ep, right).start()
        remote(own, own, ag_send.at[i, 1], ag_recv.at[i, 1], ep, left).start()

    def gather_pass(i, ref, lanes, first, count):
        (a, na), (b, nb) = parts_of(count)
        arrived(region(ref, lanes, first, count, left), ag_recv.at[i, 0])
        half = region(ref, lanes, first + a, na, left)
        remote(half, half, ag_send.at[i, 2], ag_recv.at[i, 2], ep, right).start()
        arrived(region(ref, lanes, first, count, right), ag_recv.at[i, 1])
        half = region(ref, lanes, first + b, nb, right)
        remote(half, half, ag_send.at[i, 3], ag_recv.at[i, 3], ep, left).start()

    def gather_end(i, ref, lanes, first, count):
        (a, na), (b, nb) = parts_of(count)
        arrived(region(ref, lanes, first + a, na, across), ag_recv.at[i, 2])
        arrived(region(ref, lanes, first + b, nb, across), ag_recv.at[i, 3])

    def gather_sent(i, ref, lanes, first, count):
        (a, na), (b, nb) = parts_of(count)
        left_here(region(ref, lanes, first, count, tp), ag_send.at[i, 0])
        left_here(region(ref, lanes, first, count, tp), ag_send.at[i, 1])
        left_here(region(ref, lanes, first + a, na, left), ag_send.at[i, 2])
        left_here(region(ref, lanes, first + b, nb, right), ag_send.at[i, 3])

    def rows_gather(step, group):
        step(group, xin, at_quarter, group * ROWS, ROWS)

    def hidden_gather(step, group):
        step(len(ORDER) + group, hid, at_ff, group * ROWS, ROWS)

    def come(group):
        start = group * ROWS
        if group < NEAR:
            main, rest = xin.at[start : start + BODY], in_near_rest.at[group]
        else:
            main, rest = xin.at[start : start + BODY, far_lanes()], in_far_rest.at[group - NEAR]
        sent_or_come(group, arrived, main, rest, go_recv, go_rest_recv)
        if group < NEAR:
            xin[start + BODY : start + ROWS, :] = unpack_rest(rest[...])
        else:
            xin[start + BODY : start + ROWS, far_lanes()] = unpack_rest(rest[...])

    def hidden(group):
        start = group * ROWS
        rows = xin[start : start + ROWS, :]
        value = silu(dot(rows, wg[...])) * dot(rows, wu[...])
        hid[start : start + ROWS, at_ff(tp)] = value.astype(BF16)

    def send_back(group):
        start = group * ROWS
        own = dot(hid[start : start + ROWS, :], down[...])
        back_send[group] = own[0:BODY].astype(BF16)
        back_send_rest[group] = pack_rest(own[BODY:]).astype(BF16)
        exchange(
            group,
            -1,
            back_send.at[group],
            back.at[row_of(group, mine)],
            back_send_rest.at[group],
            back_rest.at[group, mine],
            back_ssem,
            back_rsem,
            back_rest_ssem,
            back_rest_rsem,
        )
        if group == 0:
            back[row_of(0, mine), :] = back_send[0, place_rows(mine), :]
            back_rest[0, mine] = back_send_rest[0, mine]

    tall = iota((128, tokens), 0)
    wide = jnp.where(tall == 0, slot_first.astype(F32), jnp.where(tall == 1, slot_second.astype(F32), 0.0))
    loads["weights"].wait()
    given = weights_ref[...]
    wide = jnp.where(tall == 2, given[0:1, :], jnp.where(tall == 3, given[1:2, :], wide))
    turned = wide.T
    slot_one, slot_two = turned[:, 0:1].astype(jnp.int32), turned[:, 1:2].astype(jnp.int32)
    weight_one, weight_two = turned[:, 2:3], turned[:, 3:4]

    def combine(group):
        start = group * ROWS
        sent_or_come(
            group, arrived, back.at[start : start + BODY], back_rest.at[group], back_rsem, back_rest_rsem
        )
        back[start + BODY : start + ROWS, :] = unpack_rest(back_rest[group])
        lane = iota((tokens, ROWS), 1) + start
        mix = jnp.where(lane == slot_one, weight_one, 0.0) + jnp.where(lane == slot_two, weight_two, 0.0)
        high = mix.astype(BF16)
        low = (mix - high.astype(F32)).astype(BF16)
        rows = back[start : start + ROWS, :]
        total[...] += dot(high, rows) + dot(low, rows)

    arrived(halo, halo_recv)
    for b in range(blocks):
        before_rows = halo[:, b * 128 : (b + 1) * 128].astype(F32)
        padded[b, 0:extra, :] = jnp.where(ep == 0, jnp.zeros_like(before_rows), before_rows)
    ssum[...] = jnp.zeros_like(ssum)
    ssq[...] = jnp.zeros_like(ssq)

    @pl.loop(0, blocks)
    def _(b):
        for r in range(0, tokens, 64):
            acc = jnp.zeros((64, 128), F32)
            for offset in range(31):
                start = r + offset + extra - 30
                acc = acc + taps[b, offset : offset + 1, :] * padded[b, start : start + 64, :]
            conv[b, r : r + 64, :] = acc
            ssum[r : r + 64, :] += acc
            ssq[r : r + 64, :] += acc * acc

    eighth = iota((8, tokens), 0)
    sums = jnp.sum(ssum[...].T, axis=0, keepdims=True)
    squares = jnp.sum(ssq[...].T, axis=0, keepdims=True)
    own_stat = jnp.where(eighth == 0, sums, jnp.where(eighth == 1, squares, 0.0))
    stat_send[...] = own_stat
    stat[tp] = own_stat
    for i, peer in enumerate((right, left, across)):
        remote(stat_send, stat.at[tp], stat_ssem.at[i], stat_rsem.at[i], ep, peer).start()

    remote(ed.at[:, at_quarter(across)], down_rows(tp), down_send.at[2], down_recv.at[2], ep, across).start()

    loads["sg"].wait()
    loads["su"].wait()
    loads["sd"].wait()
    shared = (silu(dot(norm[...], sg[...])) * dot(norm[...], su[...])).astype(BF16)
    total[...] = dot(shared, sd[...])

    come(7)
    rows_gather(gather_start, 7)
    for i, peer in enumerate((left, right, across)):
        arrived(stat.at[peer], stat_rsem.at[i])
    sums = stat[0] + stat[1] + stat[2] + stat[3]
    average = sums[0:1] * (1.0 / width)
    variance = sums[1:2] * (1.0 / width) - average * average
    scale = lax.rsqrt(variance + epsilon)
    turned = jnp.where(tall == 0, average, jnp.where(tall == 1, scale, 0.0)).T
    average, scale = turned[:, 0:1], turned[:, 1:2]
    loads["cgain"].wait()
    for b in range(blocks):
        lanes = slice(b * 128, (b + 1) * 128)
        act[:, lanes] = silu((conv[b] - average) * scale * cgain_ref[:, lanes]).astype(BF16)

    loads["cproj"].wait()
    upper = tokens // 2
    top, bottom = slice(0, upper), slice(upper, tokens)

    def product(q):
        return dot(act[...], cproj[:, at_quarter(q)])

    cfar[...] = product(across).astype(BF16)
    cright[...] = product(right).astype(BF16)
    cleft[...] = product(left).astype(BF16)
    cown[...] = product(tp)

    remote(cfar.at[top], half_a, rs_send.at[0], rs_recv.at[0], ep, right).start()
    remote(cfar.at[bottom], half_b, rs_send.at[1], rs_recv.at[1], ep, left).start()
    come(5)
    rows_gather(gather_start, 5)
    rows_gather(gather_pass, 7)
    come(6)
    rows_gather(gather_start, 6)
    rows_gather(gather_end, 7)
    loads["wg"].wait()
    loads["wu"].wait()
    hidden(7)
    hidden_gather(gather_start, 7)
    rows_gather(gather_pass, 5)
    come(3)
    rows_gather(gather_start, 3)
    rows_gather(gather_pass, 6)
    rows_gather(gather_end, 5)
    hidden(5)
    hidden_gather(gather_start, 5)
    hidden_gather(gather_pass, 7)
    come(4)
    rows_gather(gather_start, 4)
    rows_gather(gather_pass, 3)
    rows_gather(gather_end, 6)
    hidden(6)
    hidden_gather(gather_start, 6)
    hidden_gather(gather_pass, 5)
    loads["down"].wait()
    arrived(down_rows(left), down_recv.at[0])
    arrived(down_rows(right), down_recv.at[1])
    arrived(down_rows(across), down_recv.at[2])
    hidden_gather(gather_end, 7)
    send_back(7)
    rows_gather(gather_pass, 4)
    hidden_gather(gather_pass, 6)
    rows_gather(gather_end, 3)
    hidden(3)
    hidden_gather(gather_start, 3)
    hidden_gather(gather_end, 5)
    send_back(5)
    rows_gather(gather_end, 4)
    hidden(4)
    hidden_gather(gather_start, 4)
    hidden_gather(gather_end, 6)
    send_back(6)
    hidden_gather(gather_pass, 3)
    come(2)
    hidden(2)
    hidden_gather(gather_start, 2)
    come(1)
    hidden(1)
    hidden_gather(gather_start, 1)
    hidden_gather(gather_pass, 4)
    hidden_gather(gather_end, 3)
    send_back(3)
    come(0)
    hidden(0)
    hidden_gather(gather_start, 0)
    hidden_gather(gather_end, 4)
    send_back(4)
    hidden_gather(gather_pass, 2)
    hidden_gather(gather_pass, 1)
    remote(cright.at[bottom], from_left.at[bottom], rs_send.at[2], rs_recv.at[2], ep, right).start()
    remote(cleft.at[top], from_right.at[top], rs_send.at[3], rs_recv.at[3], ep, left).start()
    hidden_gather(gather_pass, 0)
    arrived(half_a, rs_recv.at[0])
    cright[top] = (cright[top].astype(F32) + half_a[...].astype(F32)).astype(BF16)
    remote(cright.at[top], from_left.at[top], rs_send.at[4], rs_recv.at[4], ep, right).start()
    arrived(half_b, rs_recv.at[1])
    cleft[bottom] = (cleft[bottom].astype(F32) + half_b[...].astype(F32)).astype(BF16)
    remote(cleft.at[bottom], from_right.at[bottom], rs_send.at[5], rs_recv.at[5], ep, left).start()
    hidden_gather(gather_end, 2)
    send_back(2)
    hidden_gather(gather_end, 1)
    send_back(1)
    hidden_gather(gather_end, 0)
    send_back(0)
    combine(7)
    combine(5)
    combine(6)
    combine(3)
    combine(4)
    combine(2)
    combine(1)
    combine(0)
    arrived(from_left.at[bottom], rs_recv.at[2])
    arrived(from_right.at[top], rs_recv.at[3])
    arrived(from_left.at[top], rs_recv.at[4])
    arrived(from_right.at[bottom], rs_recv.at[5])
    conv_out[...] = (cown[...] + from_left[...].astype(F32) + from_right[...].astype(F32)).astype(BF16)
    moe_out[...] = total[...].astype(BF16)
    left_here(tail, halo_send)
    left_here(ed.at[:, at_quarter(right)], down_send.at[0])
    left_here(ed.at[:, at_quarter(left)], down_send.at[1])
    left_here(ed.at[:, at_quarter(across)], down_send.at[2])
    for i in range(3):
        left_here(stat_send, stat_ssem.at[i])
    for i, part in enumerate((cfar.at[top], cfar.at[bottom], cright.at[bottom], cleft.at[top], cright.at[top], cleft.at[bottom])):
        left_here(part, rs_send.at[i])
    for group in range(len(ORDER)):
        if group < NEAR:
            main, rest = send_near.at[group], send_near_rest.at[group]
        else:
            main, rest = send_far.at[group - NEAR], send_far_rest.at[group - NEAR]
        sent_or_come(group, left_here, main, rest, go_send, go_rest_send)
        sent_or_come(group, left_here, back_send.at[group], back_send_rest.at[group], back_ssem, back_rest_ssem)
        if group >= NEAR:
            rows_gather(gather_sent, group)
        hidden_gather(gather_sent, group)


def handed_on(a_ref, b_ref, a_out, b_out):
    a_out[...] = a_ref[...]
    b_out[...] = b_ref[...]


def local(
    conv_value,
    conv_gate,
    conv_taps,
    conv_gain,
    conv_proj,
    moe_tokens,
    moe_gain,
    routes,
    route_weights,
    expert_gate,
    expert_up,
    expert_down,
    shared_gate,
    shared_up,
    shared_down,
):
    tokens, width = moe_tokens.shape
    quarter = conv_value.shape[1]
    ff = expert_gate.shape[2]
    full_ff = ff * lax.axis_size("tp")
    shared_ff = shared_gate.shape[1]
    groups = len(ORDER)
    far = groups - NEAR
    hbm = pl.BlockSpec(memory_space=pl.ANY)
    vmem = pl.BlockSpec(memory_space=pltpu.VMEM)
    dma = pltpu.SemaphoreType.DMA

    def buf(*shape):
        return pltpu.VMEM(shape, BF16)

    def wide(*shape):
        return pltpu.VMEM(shape, F32)

    scratch = [
        buf(tokens, quarter),
        buf(tokens, quarter),
        buf(31, quarter),
        wide(1, quarter),
        wide(1, width),
        pltpu.VMEM((2, tokens), jnp.int32),
        wide(2, tokens),
        buf(quarter, width),
        buf(tokens, width),
        buf(width, ff),
        buf(width, ff),
        buf(width, shared_ff),
        buf(width, shared_ff),
        buf(shared_ff, quarter),
        buf(tokens, width),
        buf(NEAR, BODY, width),
        buf(NEAR, 8, 8, 512),
        buf(far, BODY, quarter),
        buf(far, 8, 8, 128),
        buf(groups * ROWS, width),
        buf(NEAR, 8, 8, 512),
        buf(far, 8, 8, 128),
        buf(groups * ROWS, full_ff),
        buf(full_ff, quarter),
        buf(groups, BODY, quarter),
        buf(groups, 8, 8, 128),
        buf(groups * ROWS, quarter),
        buf(groups, 8, 8, 128),
        wide(tokens, quarter),
        wide(quarter // 128, tokens + 32, 128),
        wide(quarter // 128, 32, 128),
        wide(quarter // 128, tokens, 128),
        wide(tokens, 128),
        wide(tokens, 128),
        buf(32, quarter),
        buf(32, quarter),
        wide(8, tokens),
        wide(4, 8, tokens),
        buf(tokens, quarter),
        buf(tokens, quarter),
        buf(tokens, quarter),
        buf(tokens, quarter),
        wide(tokens, quarter),
        buf(tokens // 2, quarter),
        buf(tokens // 2, quarter),
        buf(tokens, quarter),
        buf(tokens, quarter),
        dma((15,)),
        dma((groups,)),
        dma((groups,)),
        dma((groups,)),
        dma((groups,)),
        dma((groups,)),
        dma((groups,)),
        dma((groups,)),
        dma((groups,)),
        dma((2 * groups, 4)),
        dma((2 * groups, 4)),
        dma((3,)),
        dma((3,)),
        dma,
        dma,
        dma((3,)),
        dma((3,)),
        dma((6,)),
        dma((6,)),
    ]
    result = jax.ShapeDtypeStruct((tokens, quarter), BF16)
    results = pl.pallas_call(
        kernel,
        out_shape=(result, result),
        in_specs=[hbm] * 15,
        out_specs=(vmem, vmem),
        scratch_shapes=scratch,
        compiler_params=pltpu.CompilerParams(collective_id=0, has_side_effects=True),
    )(
        conv_value,
        conv_gate,
        conv_taps,
        conv_gain.reshape(1, -1),
        conv_proj,
        moe_tokens,
        moe_gain.reshape(1, -1),
        routes.T,
        route_weights.T,
        expert_gate,
        expert_up,
        expert_down,
        shared_gate,
        shared_up,
        shared_down,
    )
    return pl.pallas_call(
        handed_on, out_shape=(result, result), in_specs=[vmem, vmem], out_specs=(vmem, vmem)
    )(*results)


def solution(mesh):
    placed = (
        P("ep", "tp"),
        P("ep", "tp"),
        P(None, "tp"),
        P("tp"),
        P("tp", None),
        P("ep", None),
        P(),
        P("ep", None),
        P("ep", None),
        P("ep", None, "tp"),
        P("ep", None, "tp"),
        P("ep", "tp", None),
        P(),
        P(),
        P(None, "tp"),
    )
    return jax.shard_map(
        local, mesh=mesh, in_specs=placed, out_specs=(P("ep", "tp"), P("ep", "tp")), check_vma=False
    )
```

```python
import functools

import jax
import jax.numpy as jnp
from jax import lax
from jax.experimental import pallas as pl
from jax.experimental.pallas import tpu as pltpu
from jax.sharding import PartitionSpec as P

MESH = pl.DeviceIdType.MESH
F32 = jnp.float32
BF16 = jnp.bfloat16
epsilon = 1e-05

ORDER = (0, 1, 7, 2, 6, 3, 5, 4)
PLANE = 8
MAIN = 16
REST = 2
ROWS = PLANE * (MAIN + REST)
BODY = PLANE * MAIN
NEAR = 3
SENT = (7, 5, 6, 3, 4, 2, 1, 0)


def silu(v):
    return v / (1.0 + jnp.exp(-v))


def dot(a, b):
    return jnp.dot(a, b, preferred_element_type=F32)


def iota(shape, dim):
    return lax.broadcasted_iota(jnp.int32, shape, dim)


def kernel(
    cv_hbm,
    cg_hbm,
    taps_hbm,
    cgain_hbm,
    cproj_hbm,
    tok_hbm,
    mgain_hbm,
    routes_hbm,
    weights_hbm,
    eg_hbm,
    eu_hbm,
    ed_hbm,
    sg_hbm,
    su_hbm,
    sd_hbm,
    conv_out,
    moe_out,
    cv,
    cg,
    taps_ref,
    cgain_ref,
    mgain_ref,
    routes_ref,
    weights_ref,
    cproj,
    tok,
    wg,
    wu,
    sg,
    su,
    sd,
    norm,
    send_near,
    send_near_rest,
    send_far,
    send_far_rest,
    xin,
    in_near_rest,
    in_far_rest,
    hid,
    down,
    back_send,
    back_send_rest,
    back,
    back_rest,
    total,
    padded,
    taps,
    conv,
    ssum,
    ssq,
    tail,
    halo,
    stat_send,
    stat,
    act,
    cfar,
    cright,
    cleft,
    cown,
    half_a,
    half_b,
    from_left,
    from_right,
    load_sem,
    go_send,
    go_recv,
    go_rest_send,
    go_rest_recv,
    back_ssem,
    back_rsem,
    back_rest_ssem,
    back_rest_rsem,
    ag_send,
    ag_recv,
    down_send,
    down_recv,
    halo_send,
    halo_recv,
    stat_ssem,
    stat_rsem,
    rs_send,
    rs_recv,
):
    ep, tp = lax.axis_index("ep"), lax.axis_index("tp")
    n_ep, n_tp = lax.axis_size("ep"), lax.axis_size("tp")
    planes = n_ep // PLANE
    z, mine = ep // PLANE, lax.rem(ep, PLANE)
    right, left, across = (lax.rem(tp + i, n_tp) for i in (1, 3, 2))
    tokens, width = tok.shape
    quarter = width // n_tp
    ff = wg.shape[1]

    def remote(src, dst, ssem, rsem, to_ep, to_tp):
        return pltpu.make_async_remote_copy(
            src_ref=src,
            dst_ref=dst,
            send_sem=ssem,
            recv_sem=rsem,
            device_id=(to_ep, to_tp),
            device_id_type=MESH,
        )

    def arrived(ref, sem):
        remote(ref, ref, sem, sem, ep, right).wait_recv()

    def left_here(ref, sem):
        remote(ref, ref, sem, sem, ep, right).wait_send()

    barrier = pltpu.get_barrier_semaphore()

    @pl.loop(1, n_ep)
    def _(o):
        pl.semaphore_signal(
            barrier, inc=1, device_id=(lax.rem(ep + o, n_ep), tp), device_id_type=MESH
        )

    for peer in (right, left, across):
        pl.semaphore_signal(barrier, inc=1, device_id=(ep, peer), device_id_type=MESH)

    def at_quarter(q):
        return pl.ds(pl.multiple_of(q * quarter, quarter), quarter)

    def at_ff(q):
        return pl.ds(pl.multiple_of(q * ff, ff), ff)

    loads = {}
    for number, (name, src, dst) in enumerate(
        (
            ("tok", tok_hbm, tok),
            ("mgain", mgain_hbm, mgain_ref),
            ("routes", routes_hbm, routes_ref),
            ("cv", cv_hbm, cv),
            ("cg", cg_hbm, cg),
            ("taps", taps_hbm, taps_ref),
            ("cgain", cgain_hbm, cgain_ref),
            ("weights", weights_hbm, weights_ref),
            ("sg", sg_hbm, sg),
            ("su", su_hbm, su),
            ("sd", sd_hbm, sd),
            ("cproj", cproj_hbm, cproj),
            ("wg", eg_hbm.at[0], wg),
            ("wu", eu_hbm.at[0], wu),
            ("down", ed_hbm.at[0, :, at_quarter(tp)], down.at[at_ff(tp)]),
        )
    ):
        loads[name] = pltpu.make_async_copy(src, dst, load_sem.at[number])
        loads[name].start()

    loads["tok"].wait()
    loads["mgain"].wait()
    for r in range(0, tokens, 64):
        rows = tok[r : r + 64, :].astype(F32)
        mean = jnp.sum(rows, axis=1, keepdims=True) * (1.0 / width)
        centered = rows - mean
        var = jnp.sum(centered * centered, axis=1, keepdims=True) * (1.0 / width)
        norm[r : r + 64, :] = (centered * lax.rsqrt(var + epsilon) * mgain_ref[...]).astype(BF16)

    loads["routes"].wait()
    routes = routes_ref[...]
    first, second = routes[0:1, :], routes[1:2, :]
    names = iota((n_ep, tokens), 0)
    is_first = (names == first).astype(F32)
    is_second = (names == second).astype(F32)
    earlier = (iota((tokens, tokens), 0) < iota((tokens, tokens), 1)).astype(F32).astype(BF16)
    before = dot((is_first + is_second).astype(BF16), earlier)

    def slot_of(route, chosen):
        rank = jnp.sum(before * chosen, axis=0, keepdims=True).astype(jnp.int32)
        away = ((route >> 3) - z + planes) & (planes - 1)
        place = route & (PLANE - 1)
        group = jnp.where(away == 0, 0, jnp.where(away <= 4, 2 * away - 1, 2 * (planes - away)))
        inside = jnp.where(rank < MAIN, place * MAIN + rank, BODY + place * REST + rank - MAIN)
        return group * ROWS + inside

    slot_first, slot_second = slot_of(first, is_first), slot_of(second, is_second)

    way = iota((64, 64), 0)
    here = iota((64, 64), 1)
    same = (way >> 3 == (here >> 1 & 7)) & ((way >> 1 & 3) == here >> 4) & ((way & 1) == (here & 1))
    to_way = same.astype(F32).astype(BF16)
    way = iota((64, 64), 1)
    here = iota((64, 64), 0)
    same = (way >> 3 == (here >> 1 & 7)) & ((way >> 1 & 3) == here >> 4) & ((way & 1) == (here & 1))
    to_here = same.astype(F32).astype(BF16)

    def pack_rest(rest):
        n = rest.shape[1] // 512
        stacked = jnp.concatenate(
            [
                jnp.concatenate(
                    [rest[:, q * 512 + g * 128 : q * 512 + (g + 1) * 128] for q in range(n)], axis=1
                )
                for g in range(4)
            ],
            axis=0,
        )
        return dot(to_way, stacked.astype(BF16)).reshape(8, 8, n * 128)

    def unpack_rest(packed):
        n = packed.shape[2] // 128
        stacked = dot(to_here, packed.astype(F32).reshape(64, n * 128).astype(BF16))
        return jnp.concatenate(
            [
                stacked[g * 16 : (g + 1) * 16, q * 128 : (q + 1) * 128]
                for q in range(n)
                for g in range(4)
            ],
            axis=1,
        ).astype(BF16)

    def row_of(group, place, count=MAIN):
        return pl.ds(pl.multiple_of(group * ROWS + place * MAIN, MAIN), count)

    def place_rows(place):
        return pl.ds(pl.multiple_of(place * MAIN, MAIN), MAIN)

    def exchange(group, sign, main, main_at, rest, rest_at, ssem, rsem, rest_ssem, rest_rsem):
        plane = lax.rem(z + sign * ORDER[group] + planes, planes)

        @pl.loop(1 if group == 0 else 0, PLANE)
        def _(o):
            place = lax.rem(mine + o, PLANE)
            to = plane * PLANE + place
            remote(main.at[place_rows(place)], main_at, ssem.at[group], rsem.at[group], to, tp).start()
            remote(rest.at[place], rest_at, rest_ssem.at[group], rest_rsem.at[group], to, tp).start()

    def sent_or_come(group, wait, main, rest, sem, rest_sem):
        count = PLANE - 1 if group == 0 else PLANE
        wait(main.at[0 : count * MAIN], sem.at[group])
        wait(rest.at[0:count], rest_sem.at[group])

    def far_lanes():
        return at_quarter(tp)

    loads["cv"].wait()
    loads["cg"].wait()
    loads["taps"].wait()
    blocks = quarter // 128
    extra = halo.shape[0]
    for b in range(blocks):
        lanes = slice(b * 128, (b + 1) * 128)
        gated = (cv[:, lanes].astype(F32) * jax.nn.sigmoid(cg[:, lanes].astype(F32))).astype(BF16)
        padded[b, extra:, :] = gated.astype(F32)
        tail[:, lanes] = gated[tokens - extra :]
        taps[b, 0:31] = taps_ref[:, lanes].astype(F32)

    pl.semaphore_wait(barrier, n_ep - 1 + n_tp - 1)

    next_ep = lax.rem(ep + 1, n_ep)
    remote(tail, halo, halo_send, halo_recv, next_ep, tp).start()

    def down_rows(owner):
        return down.at[at_ff(owner)]

    ed = ed_hbm.at[0]
    remote(ed.at[:, at_quarter(right)], down_rows(tp), down_send.at[0], down_recv.at[0], ep, right).start()
    remote(ed.at[:, at_quarter(left)], down_rows(tp), down_send.at[1], down_recv.at[1], ep, left).start()

    for group in SENT:
        row = iota((ROWS, tokens), 0) + group * ROWS
        pick = ((row == slot_first) | (row == slot_second)).astype(F32).astype(BF16)
        if group < NEAR:
            rows = dot(pick, norm[...])
            send_near[group] = rows[0:BODY].astype(BF16)
            send_near_rest[group] = pack_rest(rows[BODY:]).astype(BF16)
            main, rest = send_near.at[group], send_near_rest.at[group]
            main_at, rest_at = xin.at[row_of(group, mine)], in_near_rest.at[group, mine]
        else:
            rows = dot(pick, norm[:, far_lanes()])
            send_far[group - NEAR] = rows[0:BODY].astype(BF16)
            send_far_rest[group - NEAR] = pack_rest(rows[BODY:]).astype(BF16)
            main, rest = send_far.at[group - NEAR], send_far_rest.at[group - NEAR]
            main_at = xin.at[row_of(group, mine), far_lanes()]
            rest_at = in_far_rest.at[group - NEAR, mine]
        exchange(group, 1, main, main_at, rest, rest_at, go_send, go_recv, go_rest_send, go_rest_recv)
        if group == 0:
            xin[row_of(0, mine), :] = send_near[0, place_rows(mine), :]
            in_near_rest[0, mine] = send_near_rest[0, mine]

    def parts_of(count):
        cut = (count // 2 + 15) // 16 * 16
        return (0, cut), (cut, count - cut)

    def region(ref, lanes, first, rows, q):
        return ref.at[first : first + rows, lanes(q)]

    def gather_start(i, ref, lanes, first, count):
        own = region(ref, lanes, first, count, tp)
        remote(own, own, ag_send.at[i, 0], ag_recv.at[i, 0], ep, right).start()
        remote(own, own, ag_send.at[i, 1], ag_recv.at[i, 1], ep, left).start()

    def gather_pass(i, ref, lanes, first, count):
        (a, na), (b, nb) = parts_of(count)
        arrived(region(ref, lanes, first, count, left), ag_recv.at[i, 0])
        half = region(ref, lanes, first + a, na, left)
        remote(half, half, ag_send.at[i, 2], ag_recv.at[i, 2], ep, right).start()
        arrived(region(ref, lanes, first, count, right), ag_recv.at[i, 1])
        half = region(ref, lanes, first + b, nb, right)
        remote(half, half, ag_send.at[i, 3], ag_recv.at[i, 3], ep, left).start()

    def gather_end(i, ref, lanes, first, count):
        (a, na), (b, nb) = parts_of(count)
        arrived(region(ref, lanes, first + a, na, across), ag_recv.at[i, 2])
        arrived(region(ref, lanes, first + b, nb, across), ag_recv.at[i, 3])

    def gather_sent(i, ref, lanes, first, count):
        (a, na), (b, nb) = parts_of(count)
        left_here(region(ref, lanes, first, count, tp), ag_send.at[i, 0])
        left_here(region(ref, lanes, first, count, tp), ag_send.at[i, 1])
        left_here(region(ref, lanes, first + a, na, left), ag_send.at[i, 2])
        left_here(region(ref, lanes, first + b, nb, right), ag_send.at[i, 3])

    def rows_gather(step, group):
        step(group, xin, at_quarter, group * ROWS, ROWS)

    def hidden_gather(step, group):
        step(len(ORDER) + group, hid, at_ff, group * ROWS, ROWS)

    def come(group):
        start = group * ROWS
        if group < NEAR:
            main, rest = xin.at[start : start + BODY], in_near_rest.at[group]
        else:
            main, rest = xin.at[start : start + BODY, far_lanes()], in_far_rest.at[group - NEAR]
        sent_or_come(group, arrived, main, rest, go_recv, go_rest_recv)
        if group < NEAR:
            xin[start + BODY : start + ROWS, :] = unpack_rest(rest[...])
        else:
            xin[start + BODY : start + ROWS, far_lanes()] = unpack_rest(rest[...])

    def hidden(group):
        start = group * ROWS
        rows = xin[start : start + ROWS, :]
        value = silu(dot(rows, wg[...])) * dot(rows, wu[...])
        hid[start : start + ROWS, at_ff(tp)] = value.astype(BF16)

    def send_back(group):
        start = group * ROWS
        own = dot(hid[start : start + ROWS, :], down[...])
        back_send[group] = own[0:BODY].astype(BF16)
        back_send_rest[group] = pack_rest(own[BODY:]).astype(BF16)
        exchange(
            group,
            -1,
            back_send.at[group],
            back.at[row_of(group, mine)],
            back_send_rest.at[group],
            back_rest.at[group, mine],
            back_ssem,
            back_rsem,
            back_rest_ssem,
            back_rest_rsem,
        )
        if group == 0:
            back[row_of(0, mine), :] = back_send[0, place_rows(mine), :]
            back_rest[0, mine] = back_send_rest[0, mine]

    tall = iota((128, tokens), 0)
    wide = jnp.where(tall == 0, slot_first.astype(F32), jnp.where(tall == 1, slot_second.astype(F32), 0.0))
    loads["weights"].wait()
    given = weights_ref[...]
    wide = jnp.where(tall == 2, given[0:1, :], jnp.where(tall == 3, given[1:2, :], wide))
    turned = wide.T
    slot_one, slot_two = turned[:, 0:1].astype(jnp.int32), turned[:, 1:2].astype(jnp.int32)
    weight_one, weight_two = turned[:, 2:3], turned[:, 3:4]

    def combine(group):
        start = group * ROWS
        sent_or_come(
            group, arrived, back.at[start : start + BODY], back_rest.at[group], back_rsem, back_rest_rsem
        )
        back[start + BODY : start + ROWS, :] = unpack_rest(back_rest[group])
        lane = iota((tokens, ROWS), 1) + start
        mix = jnp.where(lane == slot_one, weight_one, 0.0) + jnp.where(lane == slot_two, weight_two, 0.0)
        high = mix.astype(BF16)
        low = (mix - high.astype(F32)).astype(BF16)
        rows = back[start : start + ROWS, :]
        total[...] += dot(high, rows) + dot(low, rows)

    arrived(halo, halo_recv)
    for b in range(blocks):
        before_rows = halo[:, b * 128 : (b + 1) * 128].astype(F32)
        padded[b, 0:extra, :] = jnp.where(ep == 0, jnp.zeros_like(before_rows), before_rows)
    ssum[...] = jnp.zeros_like(ssum)
    ssq[...] = jnp.zeros_like(ssq)

    @pl.loop(0, blocks)
    def _(b):
        for r in range(0, tokens, 64):
            acc = jnp.zeros((64, 128), F32)
            for offset in range(31):
                start = r + offset + extra - 30
                acc = acc + taps[b, offset : offset + 1, :] * padded[b, start : start + 64, :]
            conv[b, r : r + 64, :] = acc
            ssum[r : r + 64, :] += acc
            ssq[r : r + 64, :] += acc * acc

    eighth = iota((8, tokens), 0)
    sums = jnp.sum(ssum[...].T, axis=0, keepdims=True)
    squares = jnp.sum(ssq[...].T, axis=0, keepdims=True)
    own_stat = jnp.where(eighth == 0, sums, jnp.where(eighth == 1, squares, 0.0))
    stat_send[...] = own_stat
    stat[tp] = own_stat
    for i, peer in enumerate((right, left, across)):
        remote(stat_send, stat.at[tp], stat_ssem.at[i], stat_rsem.at[i], ep, peer).start()

    remote(ed.at[:, at_quarter(across)], down_rows(tp), down_send.at[2], down_recv.at[2], ep, across).start()

    loads["sg"].wait()
    loads["su"].wait()
    loads["sd"].wait()
    shared = (silu(dot(norm[...], sg[...])) * dot(norm[...], su[...])).astype(BF16)
    total[...] = dot(shared, sd[...])

    come(7)
    rows_gather(gather_start, 7)
    for i, peer in enumerate((left, right, across)):
        arrived(stat.at[peer], stat_rsem.at[i])
    sums = stat[0] + stat[1] + stat[2] + stat[3]
    average = sums[0:1] * (1.0 / width)
    variance = sums[1:2] * (1.0 / width) - average * average
    scale = lax.rsqrt(variance + epsilon)
    turned = jnp.where(tall == 0, average, jnp.where(tall == 1, scale, 0.0)).T
    average, scale = turned[:, 0:1], turned[:, 1:2]
    loads["cgain"].wait()
    for b in range(blocks):
        lanes = slice(b * 128, (b + 1) * 128)
        act[:, lanes] = silu((conv[b] - average) * scale * cgain_ref[:, lanes]).astype(BF16)

    loads["cproj"].wait()
    upper = tokens // 2
    top, bottom = slice(0, upper), slice(upper, tokens)

    def product(q):
        return dot(act[...], cproj[:, at_quarter(q)])

    cfar[...] = product(across).astype(BF16)
    cright[...] = product(right).astype(BF16)
    cleft[...] = product(left).astype(BF16)
    cown[...] = product(tp)

    remote(cfar.at[top], half_a, rs_send.at[0], rs_recv.at[0], ep, right).start()
    remote(cfar.at[bottom], half_b, rs_send.at[1], rs_recv.at[1], ep, left).start()
    rows_gather(gather_pass, 7)
    come(5)
    rows_gather(gather_start, 5)
    come(6)
    rows_gather(gather_start, 6)
    rows_gather(gather_end, 7)
    loads["wg"].wait()
    loads["wu"].wait()
    hidden(7)
    hidden_gather(gather_start, 7)
    rows_gather(gather_pass, 5)
    come(4)
    rows_gather(gather_start, 4)
    rows_gather(gather_pass, 6)
    rows_gather(gather_end, 5)
    hidden(5)
    hidden_gather(gather_start, 5)
    hidden_gather(gather_pass, 7)
    come(3)
    rows_gather(gather_start, 3)
    rows_gather(gather_end, 6)
    hidden(6)
    hidden_gather(gather_start, 6)
    loads["down"].wait()
    arrived(down_rows(left), down_recv.at[0])
    arrived(down_rows(right), down_recv.at[1])
    arrived(down_rows(across), down_recv.at[2])
    hidden_gather(gather_end, 7)
    send_back(7)
    rows_gather(gather_pass, 4)
    hidden_gather(gather_pass, 5)
    hidden_gather(gather_pass, 6)
    come(1)
    hidden(1)
    hidden_gather(gather_start, 1)
    rows_gather(gather_pass, 3)
    hidden_gather(gather_end, 5)
    send_back(5)
    hidden_gather(gather_end, 6)
    send_back(6)
    rows_gather(gather_end, 4)
    hidden(4)
    hidden_gather(gather_start, 4)
    hidden_gather(gather_pass, 1)
    come(2)
    hidden(2)
    hidden_gather(gather_start, 2)
    rows_gather(gather_end, 3)
    hidden(3)
    hidden_gather(gather_start, 3)
    hidden_gather(gather_pass, 4)
    come(0)
    hidden(0)
    hidden_gather(gather_start, 0)
    hidden_gather(gather_pass, 3)
    hidden_gather(gather_end, 1)
    send_back(1)
    hidden_gather(gather_end, 4)
    send_back(4)
    hidden_gather(gather_pass, 2)
    combine(7)
    hidden_gather(gather_pass, 0)
    remote(cright.at[bottom], from_left.at[bottom], rs_send.at[2], rs_recv.at[2], ep, right).start()
    remote(cleft.at[top], from_right.at[top], rs_send.at[3], rs_recv.at[3], ep, left).start()
    hidden_gather(gather_end, 3)
    send_back(3)
    hidden_gather(gather_end, 2)
    send_back(2)
    arrived(half_a, rs_recv.at[0])
    cright[top] = (cright[top].astype(F32) + half_a[...].astype(F32)).astype(BF16)
    remote(cright.at[top], from_left.at[top], rs_send.at[4], rs_recv.at[4], ep, right).start()
    arrived(half_b, rs_recv.at[1])
    cleft[bottom] = (cleft[bottom].astype(F32) + half_b[...].astype(F32)).astype(BF16)
    remote(cleft.at[bottom], from_right.at[bottom], rs_send.at[5], rs_recv.at[5], ep, left).start()
    hidden_gather(gather_end, 0)
    send_back(0)
    combine(4)
    combine(5)
    combine(6)
    combine(1)
    combine(0)
    combine(3)
    arrived(from_left.at[bottom], rs_recv.at[2])
    arrived(from_right.at[top], rs_recv.at[3])
    arrived(from_left.at[top], rs_recv.at[4])
    arrived(from_right.at[bottom], rs_recv.at[5])
    conv_out[...] = (cown[...] + from_left[...].astype(F32) + from_right[...].astype(F32)).astype(BF16)
    combine(2)
    moe_out[...] = total[...].astype(BF16)
    left_here(tail, halo_send)
    left_here(ed.at[:, at_quarter(right)], down_send.at[0])
    left_here(ed.at[:, at_quarter(left)], down_send.at[1])
    left_here(ed.at[:, at_quarter(across)], down_send.at[2])
    for i in range(3):
        left_here(stat_send, stat_ssem.at[i])
    for i, part in enumerate((cfar.at[top], cfar.at[bottom], cright.at[bottom], cleft.at[top], cright.at[top], cleft.at[bottom])):
        left_here(part, rs_send.at[i])
    for group in range(len(ORDER)):
        if group < NEAR:
            main, rest = send_near.at[group], send_near_rest.at[group]
        else:
            main, rest = send_far.at[group - NEAR], send_far_rest.at[group - NEAR]
        sent_or_come(group, left_here, main, rest, go_send, go_rest_send)
        sent_or_come(group, left_here, back_send.at[group], back_send_rest.at[group], back_ssem, back_rest_ssem)
        if group >= NEAR:
            rows_gather(gather_sent, group)
        hidden_gather(gather_sent, group)


def handed_on(a_ref, b_ref, a_out, b_out):
    a_out[...] = a_ref[...]
    b_out[...] = b_ref[...]


def local(
    conv_value,
    conv_gate,
    conv_taps,
    conv_gain,
    conv_proj,
    moe_tokens,
    moe_gain,
    routes,
    route_weights,
    expert_gate,
    expert_up,
    expert_down,
    shared_gate,
    shared_up,
    shared_down,
):
    tokens, width = moe_tokens.shape
    quarter = conv_value.shape[1]
    ff = expert_gate.shape[2]
    full_ff = ff * lax.axis_size("tp")
    shared_ff = shared_gate.shape[1]
    groups = len(ORDER)
    far = groups - NEAR
    hbm = pl.BlockSpec(memory_space=pl.ANY)
    vmem = pl.BlockSpec(memory_space=pltpu.VMEM)
    dma = pltpu.SemaphoreType.DMA

    def buf(*shape):
        return pltpu.VMEM(shape, BF16)

    def wide(*shape):
        return pltpu.VMEM(shape, F32)

    scratch = [
        buf(tokens, quarter),
        buf(tokens, quarter),
        buf(31, quarter),
        wide(1, quarter),
        wide(1, width),
        pltpu.VMEM((2, tokens), jnp.int32),
        wide(2, tokens),
        buf(quarter, width),
        buf(tokens, width),
        buf(width, ff),
        buf(width, ff),
        buf(width, shared_ff),
        buf(width, shared_ff),
        buf(shared_ff, quarter),
        buf(tokens, width),
        buf(NEAR, BODY, width),
        buf(NEAR, 8, 8, 512),
        buf(far, BODY, quarter),
        buf(far, 8, 8, 128),
        buf(groups * ROWS, width),
        buf(NEAR, 8, 8, 512),
        buf(far, 8, 8, 128),
        buf(groups * ROWS, full_ff),
        buf(full_ff, quarter),
        buf(groups, BODY, quarter),
        buf(groups, 8, 8, 128),
        buf(groups * ROWS, quarter),
        buf(groups, 8, 8, 128),
        wide(tokens, quarter),
        wide(quarter // 128, tokens + 32, 128),
        wide(quarter // 128, 32, 128),
        wide(quarter // 128, tokens, 128),
        wide(tokens, 128),
        wide(tokens, 128),
        buf(32, quarter),
        buf(32, quarter),
        wide(8, tokens),
        wide(4, 8, tokens),
        buf(tokens, quarter),
        buf(tokens, quarter),
        buf(tokens, quarter),
        buf(tokens, quarter),
        wide(tokens, quarter),
        buf(tokens // 2, quarter),
        buf(tokens // 2, quarter),
        buf(tokens, quarter),
        buf(tokens, quarter),
        dma((15,)),
        dma((groups,)),
        dma((groups,)),
        dma((groups,)),
        dma((groups,)),
        dma((groups,)),
        dma((groups,)),
        dma((groups,)),
        dma((groups,)),
        dma((2 * groups, 4)),
        dma((2 * groups, 4)),
        dma((3,)),
        dma((3,)),
        dma,
        dma,
        dma((3,)),
        dma((3,)),
        dma((6,)),
        dma((6,)),
    ]
    result = jax.ShapeDtypeStruct((tokens, quarter), BF16)
    results = pl.pallas_call(
        kernel,
        out_shape=(result, result),
        in_specs=[hbm] * 15,
        out_specs=(vmem, vmem),
        scratch_shapes=scratch,
        compiler_params=pltpu.CompilerParams(collective_id=0, has_side_effects=True),
    )(
        conv_value,
        conv_gate,
        conv_taps,
        conv_gain.reshape(1, -1),
        conv_proj,
        moe_tokens,
        moe_gain.reshape(1, -1),
        routes.T,
        route_weights.T,
        expert_gate,
        expert_up,
        expert_down,
        shared_gate,
        shared_up,
        shared_down,
    )
    return pl.pallas_call(
        handed_on, out_shape=(result, result), in_specs=[vmem, vmem], out_specs=(vmem, vmem)
    )(*results)


def solution(mesh):
    placed = (
        P("ep", "tp"),
        P("ep", "tp"),
        P(None, "tp"),
        P("tp"),
        P("tp", None),
        P("ep", None),
        P(),
        P("ep", None),
        P("ep", None),
        P("ep", None, "tp"),
        P("ep", None, "tp"),
        P("ep", "tp", None),
        P(),
        P(),
        P(None, "tp"),
    )
    return jax.shard_map(
        local, mesh=mesh, in_specs=placed, out_specs=(P("ep", "tp"), P("ep", "tp")), check_vma=False
    )
```
